32 devices in a mesh: fs: 8 (over z, x), tp: 4 (over y, core).
Axes of the slice: x: 2, y: 2, z: 4, core: 2. Of those that a mesh axis runs over, the one named last changes fastest.
Arguments:
- tokens: bfloat16 [4096, 2048], P('fs', 'tp'), may hold values from -6 to 6
- pre_gain: float32 [2048], replicated, may hold values from 0.1 to 1.9
- pre_gate: float32 [2048, 2816], P('fs', 'tp'), may hold values from -0.125 to 0.125
- pre_up: float32 [2048, 2816], P('fs', 'tp'), may hold values from -0.125 to 0.125
- pre_down: float32 [2816, 2048], P('fs', 'tp'), may hold values from -0.109375 to 0.109375
- mix_gain: float32 [2048], replicated, may hold values from 0.1 to 1.9
- branch_proj: float32 [2048, 1024], P('fs', 'tp'), may hold values from -0.125 to 0.125
- gate_proj: float32 [2048, 1024], P('fs', 'tp'), may hold values from -0.125 to 0.125
- conv_taps: float32 [4, 1024], P(None, 'tp'), may hold values from -3 to 3
- retain_blocks: float32 [16, 64, 64], P('tp'), may hold values from -0.75 to 0.75
- admit_blocks: float32 [16, 64, 64], P('tp'), may hold values from -0.75 to 0.75
- decay_param: float32 [1024], P('tp'), may hold values from 5 to 8.5
- channel_gain: float32 [1024], replicated, may hold values from 0.1 to 1.9
- out_proj: float32 [1024, 2048], P('fs', 'tp'), may hold values from -0.1875 to 0.1875
- post_gain: float32 [2048], replicated, may hold values from 0.1 to 1.9
- post_gate: float32 [2048, 2816], P('fs', 'tp'), may hold values from -0.125 to 0.125
- post_up: float32 [2048, 2816], P('fs', 'tp'), may hold values from -0.125 to 0.125
- post_down: float32 [2816, 2048], P('fs', 'tp'), may hold values from -0.109375 to 0.109375
Outputs:
- layer_out: bfloat16 [4096, 2048], P('fs', 'tp')
The draws below stay inside these ranges and needn't reach their ends.
All inputs are finite; a program needn't handle non-finite values.
Results may differ from the reference program's by a relative error of at most 0.012.
Values may be sent and summed in bfloat16 or wider, within the bound.
A program may use at most 64 MiB of HBM per device.

```python
import jax
import jax.numpy as jnp
from jax import lax

D = 2048
FF = 2816
HEADS = 16
BLOCK = 64
CONV = 4
SEQ_LEN = 128
DL = 1024
TOKENS = 4096


def block_levels(key, dims, shards, least, largest):
    factor_of = 1.0
    for dim, blocks in shards:
        draws = jax.random.uniform(jax.random.fold_in(jax.random.fold_in(key, 6), dim), (blocks,), jnp.float32, least / len(shards), largest / len(shards))
        factor_of = factor_of * jnp.repeat(jnp.exp(draws), dims[dim] // blocks).reshape((-1,) + (1,) * (len(dims) - 1 - dim))
    return factor_of


def noise(key, shape, scale, bound, cuts=(), held_as=jnp.bfloat16):
    level = block_levels(key, shape, cuts, -0.22, 0.18) if cuts else 1.0
    result = jax.random.normal(key, shape, jnp.float32) * scale * level
    return jnp.minimum(jnp.maximum(result, -bound), bound).astype(held_as)


def setup_inputs(seed: int = 0) -> dict:
    streams_of = jax.random.split(jax.random.key(seed), 19)
    return {
        "tokens": noise(streams_of[0], (TOKENS, D), 1.0, 6.0, ((0, 8), (1, 4))),
        "pre_gain": jnp.clip(1.0 + 0.18 * jax.random.normal(streams_of[1], (D,), jnp.float32), 0.1, 1.9),
        "pre_gate": noise(streams_of[2], (D, FF), D ** -0.5, 0.125, ((0, 8), (1, 4)), jnp.float32),
        "pre_up": noise(streams_of[3], (D, FF), D ** -0.5, 0.125, ((0, 8), (1, 4)), jnp.float32),
        "pre_down": noise(streams_of[4], (FF, D), FF ** -0.5, 0.109375, ((0, 8), (1, 4)), jnp.float32),
        "mix_gain": jnp.clip(1.0 + 0.18 * jax.random.normal(streams_of[5], (D,), jnp.float32), 0.1, 1.9),
        "branch_proj": noise(streams_of[6], (D, DL), D ** -0.5, 0.125, ((0, 8), (1, 4)), jnp.float32),
        "gate_proj": noise(streams_of[7], (D, DL), D ** -0.5, 0.125, ((0, 8), (1, 4)), jnp.float32),
        "conv_taps": noise(streams_of[8], (CONV, DL), CONV ** -0.5, 3.0, ((1, 4),), jnp.float32),
        "retain_blocks": noise(streams_of[9], (HEADS, BLOCK, BLOCK), BLOCK ** -0.5, 0.75, ((0, 4),), jnp.float32),
        "admit_blocks": noise(streams_of[10], (HEADS, BLOCK, BLOCK), BLOCK ** -0.5, 0.75, ((0, 4),), jnp.float32),
        "decay_param": jnp.clip(5.0 + 3.5 * jax.random.uniform(streams_of[11], (DL,), jnp.float32) ** block_levels(streams_of[11], (DL,), ((0, 4),), -0.2, 0.2), 5.0, 8.5),
        "channel_gain": jnp.clip(1.0 + 0.18 * jax.random.normal(streams_of[12], (DL,), jnp.float32), 0.1, 1.9),
        "out_proj": noise(streams_of[13], (DL, D), DL ** -0.5, 0.1875, ((0, 8), (1, 4)), jnp.float32),
        "post_gain": jnp.clip(1.0 + 0.18 * jax.random.normal(streams_of[14], (D,), jnp.float32), 0.1, 1.9),
        "post_gate": noise(streams_of[15], (D, FF), D ** -0.5, 0.125, ((0, 8), (1, 4)), jnp.float32),
        "post_up": noise(streams_of[16], (D, FF), D ** -0.5, 0.125, ((0, 8), (1, 4)), jnp.float32),
        "post_down": noise(streams_of[17], (FF, D), FF ** -0.5, 0.109375, ((0, 8), (1, 4)), jnp.float32),
    }


EPSILON = 1e-06
DECAY_SCALE = 8.0

def normalize(values, norm_gain):
    floats = values.astype(jnp.float32)
    scaled = floats * lax.rsqrt(lax.optimization_barrier(jnp.mean(floats * floats, axis=-1, keepdims=True)) + EPSILON)
    return (scaled * norm_gain).astype(jnp.bfloat16)

def product(operand, matrix):
    return jnp.dot(operand, matrix.astype(jnp.bfloat16), preferred_element_type=jnp.float32)

def combine(earlier, latter):
    keep_early, add_early = earlier
    keep_late, add_late = latter
    return (keep_early * keep_late, keep_late * add_early + add_late)

def feed_forward(residual, norm_gain, gate_matrix, up_matrix, down_matrix):
    normed = normalize(residual, norm_gain)
    hidden = (jax.nn.silu(product(normed, gate_matrix)) * product(normed, up_matrix)).astype(jnp.bfloat16)
    return (residual.astype(jnp.float32) + 0.5 * product(hidden, down_matrix)).astype(jnp.bfloat16)

def block_gate(convolved, blocks):
    rounded = lax.optimization_barrier(blocks.astype(jnp.bfloat16)).astype(jnp.float32)
    grouped = convolved.astype(jnp.float32).reshape(convolved.shape[0], convolved.shape[1], blocks.shape[0], blocks.shape[1])
    mixed = jnp.einsum('sthi,hij->sthj', grouped, rounded)
    return jax.nn.sigmoid(mixed).reshape(convolved.shape)

def recurrent_mixer(residual, norm_gain, branch_matrix, gate_matrix, conv_taps, retain_blocks, admit_blocks, decay_param, channel_gain, out_matrix):
    normed = normalize(residual, norm_gain)
    branch = product(normed, branch_matrix)
    gate_act = product(normed, gate_matrix)
    sequences = residual.shape[0] // SEQ_LEN
    channel_count = branch.shape[1]
    framed = branch.reshape(sequences, SEQ_LEN, channel_count)
    padded = jnp.pad(framed, ((0, 0), (CONV - 1, 0), (0, 0)))
    convolved = jnp.zeros_like(framed)
    for tap_index in range(CONV):
        convolved = convolved + padded[:, tap_index:tap_index + SEQ_LEN] * conv_taps[tap_index]
    convolved = convolved.astype(jnp.bfloat16)
    retained = block_gate(convolved, retain_blocks)
    admitted = block_gate(convolved, admit_blocks)
    log_keep = -DECAY_SCALE * retained * jax.nn.softplus(-decay_param)
    inject = jnp.sqrt(-jnp.expm1(2.0 * log_keep)) * admitted * convolved.astype(jnp.float32)
    _, states = lax.associative_scan(combine, (jnp.exp(log_keep), inject), axis=1)
    mixed_rows = (states.reshape(residual.shape[0], channel_count) * jax.nn.gelu(gate_act)).astype(jnp.bfloat16)
    mixed_normed = normalize(mixed_rows, channel_gain)
    return (residual.astype(jnp.float32) + product(mixed_normed, out_matrix)).astype(jnp.bfloat16)

def reference(tokens, pre_gain, pre_gate, pre_up, pre_down, mix_gain, branch_proj, gate_proj, conv_taps, retain_blocks, admit_blocks, decay_param, channel_gain, out_proj, post_gain, post_gate, post_up, post_down):
    after_pre = feed_forward(tokens, pre_gain, pre_gate, pre_up, pre_down)
    after_mix = recurrent_mixer(after_pre, mix_gain, branch_proj, gate_proj, conv_taps, retain_blocks, admit_blocks, decay_param, channel_gain, out_proj)
    return feed_forward(after_mix, post_gain, post_gate, post_up, post_down)
```

```python
import functools

import jax
import jax.numpy as jnp
from jax import lax
from jax.experimental import pallas as pl
from jax.experimental.pallas import tpu as pltpu
from jax.sharding import PartitionSpec as P

SEQ_LEN = 128


EPSILON = 1e-06
DECAY_SCALE = 8.0


def normalize(values, norm_gain):
    floats = values.astype(jnp.float32)
    scaled = floats * lax.rsqrt(jnp.mean(floats * floats, axis=-1, keepdims=True) + EPSILON)
    return (scaled * norm_gain).astype(jnp.bfloat16)


def widen(residual):
    return lax.all_gather(residual, "tp", axis=1, tiled=True)


def contract(operand, stacked):
    return jnp.dot(
        operand,
        lax.all_gather(stacked.astype(jnp.bfloat16), "fs", axis=0, tiled=True),
        preferred_element_type=jnp.float32,
    )


def feed_forward(residual, norm_gain, gate_matrix, up_matrix, down_matrix):
    normed = normalize(widen(residual), norm_gain)
    products = contract(normed, jnp.concatenate((gate_matrix, up_matrix), axis=1))
    split_at = gate_matrix.shape[1]
    hidden = (jax.nn.silu(products[:, :split_at]) * products[:, split_at:]).astype(jnp.bfloat16)
    all_hidden = lax.all_gather(hidden, "tp", axis=1, tiled=True)
    return (residual.astype(jnp.float32) + 0.5 * contract(all_hidden, down_matrix)).astype(
        jnp.bfloat16
    )


def shifted(values, distance, fill):
    row = lax.broadcasted_iota(jnp.int32, values.shape, 0)
    return jnp.where(row >= distance, pltpu.roll(values, distance, 0), fill)


def mix_sequence(branch, gate_act, taps, gates, sharpness):
    width = branch.shape[1]
    count = taps.shape[0]
    convolved = branch * taps[count - 1 : count]
    for back in range(1, count):
        convolved = convolved + shifted(branch, back, 0.0) * taps[count - 1 - back : count - back]
    convolved = convolved.astype(jnp.bfloat16)
    both = jax.nn.sigmoid(jnp.dot(convolved, gates, preferred_element_type=jnp.float32))
    log_keep = -DECAY_SCALE * both[:, :width] * sharpness
    keep = jnp.exp(log_keep)
    inject = (
        jnp.sqrt(jnp.tanh(-log_keep) * (1.0 + keep * keep))
        * both[:, width:]
        * convolved.astype(jnp.float32)
    )
    distance = 1
    while distance < branch.shape[0]:
        inject = keep * shifted(inject, distance, 0.0) + inject
        keep = keep * shifted(keep, distance, 1.0)
        distance *= 2
    return (inject * jax.nn.gelu(gate_act)).astype(jnp.bfloat16)


def mix_kernel(products_ref, taps_ref, gates_ref, sharp_ref, out_ref):
    width = out_ref.shape[1]
    out_ref[...] = mix_sequence(
        products_ref[:, :width],
        products_ref[:, width:],
        taps_ref[...],
        gates_ref[...],
        sharp_ref[...],
    )


def spread_blocks(blocks):
    count, size, _ = blocks.shape
    eye = jnp.eye(count, dtype=blocks.dtype)
    wide = eye[:, None, :, None] * blocks[:, :, None, :]
    return wide.reshape(count * size, count * size).astype(jnp.bfloat16)


def recurrent_mixer(
    residual,
    norm_gain,
    branch_matrix,
    gate_matrix,
    conv_taps,
    retain_blocks,
    admit_blocks,
    decay_param,
    channel_gain,
    out_matrix,
):
    normed = normalize(widen(residual), norm_gain)
    products = contract(normed, jnp.concatenate((branch_matrix, gate_matrix), axis=1))
    width = branch_matrix.shape[1]
    rows = residual.shape[0]
    gates = jnp.concatenate((spread_blocks(retain_blocks), spread_blocks(admit_blocks)), axis=1)
    sharpness = jax.nn.softplus(-decay_param)[None, :]
    whole = lambda array: pl.BlockSpec(array.shape, lambda i: (0, 0))
    mixed_rows = pl.pallas_call(
        mix_kernel,
        grid=(rows // SEQ_LEN,),
        in_specs=[
            pl.BlockSpec((SEQ_LEN, 2 * width), lambda i: (i, 0)),
            whole(conv_taps),
            whole(gates),
            whole(sharpness),
        ],
        out_specs=pl.BlockSpec((SEQ_LEN, width), lambda i: (i, 0)),
        out_shape=jax.ShapeDtypeStruct((rows, width), jnp.bfloat16),
        cost_estimate=pl.CostEstimate(
            flops=rows * width * 1200, bytes_accessed=rows * width * 10, transcendentals=0
        ),
    )(products, conv_taps, gates, sharpness)
    all_channels = lax.all_gather(mixed_rows, "tp", axis=1, tiled=True)
    mixed_normed = normalize(all_channels, channel_gain)
    return (residual.astype(jnp.float32) + contract(mixed_normed, out_matrix)).astype(jnp.bfloat16)


TILE = SEQ_LEN
MESH = pl.DeviceIdType.MESH


def when(condition, action):
    if condition is None:
        action()
    else:
        pl.when(condition)(action)


class Exchange:
    def __init__(self):
        self.sent = []

    def send(self, source, target, send_sem, recv_sem, device, condition=None):
        copy = remote(source, target, send_sem, recv_sem, device)
        when(condition, copy.start)
        self.sent.append((copy, condition))

    def drain(self):
        for copy, condition in self.sent:
            when(condition, copy.wait_send)


def remote(source, target, send_sem, recv_sem, device):
    return pltpu.make_async_remote_copy(
        src_ref=source,
        dst_ref=target,
        send_sem=send_sem,
        recv_sem=recv_sem,
        device_id=device,
        device_id_type=MESH,
    )


def layer_kernel(fs_size, tp_size, *refs):
    (tokens, pre_gain, mix_gain, channel_gain, post_gain) = refs[:5]
    own_side = refs[5:8]
    shards = refs[8:16]
    out = refs[16]
    whole = refs[17:25]
    first, second, third, hidden_one, hidden_two, channels = refs[25:31]
    normed, gate_part, final = refs[31:34]
    side = refs[34:37]
    recv_sem, up_sem, down_sem, far_sem, pair_sem, swap_sem, keep_sem = refs[37:44]
    token_sem, token_recv, token_pass = refs[44:47]
    slot_recv, x_sem, y_sem, pass_sem = refs[47:51]
    side_sem, side_recv, out_sem, out_recv = refs[51:55]
    taps, gates, sharpness = side

    f = lax.axis_index("fs")
    t = lax.axis_index("tp")
    x = lax.rem(f, 2)
    z = f // 2
    y = t // 2
    c = lax.rem(t, 2)
    depth = fs_size // 2
    home = x == c
    away = x != c
    end = (z == 0) | (z == depth - 1)
    inner = (z > 0) & (z < depth - 1)

    mine = 2 * y + x
    beside = 2 * y + 1 - x
    behind = 2 * (1 - y) + x
    corner = 2 * (1 - y) + 1 - x
    line = 2 * z + c

    across = f + 1 - 2 * x
    other = t + 1 - 2 * c
    x_peer = {"fs": across}
    y_peer = {"tp": lax.rem(t + 2, tp_size)}
    twin = {"tp": other}
    partner = {"fs": across, "tp": other}
    skew = {"tp": lax.rem(other + 2, tp_size)}
    above = {"fs": lax.rem(f + 2, fs_size)}
    below = {"fs": lax.rem(f + fs_size - 2, fs_size)}
    above_two = {"fs": lax.rem(f + 4, fs_size)}
    below_two = {"fs": lax.rem(f + fs_size - 4, fs_size)}
    links = Exchange()

    barrier = pltpu.get_barrier_semaphore()
    greeted = [
        (x_peer, None),
        (y_peer, None),
        (twin, None),
        (partner, None),
        (skew, None),
        (above, z < depth - 1),
        (below, z > 0),
        (above_two, z < depth - 2),
        (below_two, z > 1),
    ]
    expected = 0
    for device, condition in greeted:
        when(
            condition,
            functools.partial(
                pl.semaphore_signal, barrier, inc=1, device_id=device, device_id_type=MESH
            ),
        )
        expected = expected + (1 if condition is None else condition.astype(jnp.int32))
    pl.semaphore_wait(barrier, expected)

    def block(p, owner):
        rows = shards[p].shape[0]
        return whole[p].at[pl.ds(pl.multiple_of(owner * rows, rows), rows)]

    def arrive(p, owner, condition=None):
        place = block(p, owner)
        copy = remote(place, place, pair_sem.at[p, 0], recv_sem.at[p, owner], twin)
        when(condition, copy.wait_recv)

    def swap(p):
        links.send(
            shards[p], block(p, f), swap_sem.at[p], recv_sem.at[p, f], partner, away
        )
        when(home, pltpu.make_async_copy(shards[p], block(p, f), keep_sem.at[p]).start)

    def settle(p):
        when(home, pltpu.make_async_copy(shards[p], block(p, f), keep_sem.at[p]).wait)
        arrive(p, line, away)

    def launch(p):
        place, sem = block(p, line), recv_sem.at[p, line]
        links.send(place, place, far_sem.at[p, 0], sem, above_two, z == 0)
        links.send(place, place, far_sem.at[p, 1], sem, below_two, z == depth - 1)
        links.send(place, place, up_sem.at[p, z], sem, above, z < depth - 2)
        links.send(place, place, down_sem.at[p, z], sem, below, z > 1)
        links.send(place, place, pair_sem.at[p, z], sem, twin)

    def launch_last(p):
        place, sem = block(p, line), recv_sem.at[p, line]
        up_sem_index, down_sem_index = z, z
        links.send(place, place, up_sem.at[p, up_sem_index], sem, above, z == depth - 2)
        links.send(place, place, down_sem.at[p, down_sem_index], sem, below, z == 1)

    def take(p, level, condition):
        owner = 2 * level + c
        arrive(p, owner, condition)
        place, sem = block(p, owner), recv_sem.at[p, owner]
        upward = condition & (z > 1) & (z < depth - 1) & (level < z)
        downward = condition & (z < depth - 2) & (z > 0) & (level > z)
        links.send(place, place, up_sem.at[p, level], sem, above, upward)
        links.send(place, place, down_sem.at[p, level], sem, below, downward)
        links.send(place, place, pair_sem.at[p, level], sem, twin, condition)

    def pump(p, condition):
        for distance in range(1, depth):
            for sign in (-1, 1):
                level = z + sign * distance
                exists = (level >= 0) & (level < depth)
                take(p, lax.rem(level + depth, depth), condition & exists)

    def ready(p):
        pump(p, end)
        for level in range(depth):
            arrive(p, 2 * level + 1 - c)

    def tile_rows(s):
        return pl.ds(pl.multiple_of(s * TILE, TILE), TILE)

    def tile_sends(array, index, s):
        rows = tile_rows(s)
        place, sem = array.at[mine, rows], slot_recv.at[index, mine, s]
        return (
            remote(place, place, x_sem.at[index, s], sem, x_peer),
            remote(place, place, y_sem.at[index, s], sem, y_peer),
        )

    def tile_pass(array, index, s):
        odd = lax.rem(s, 2)
        slot = behind * (1 - odd) + beside * odd
        place = array.at[slot, tile_rows(s)]
        device = {
            "fs": f + (1 - odd) * (1 - 2 * x),
            "tp": lax.rem(t + 2 * odd, tp_size),
        }
        return remote(
            place, place, pass_sem.at[index, s], slot_recv.at[index, slot, s], device
        )

    def emit(array, index, s):
        for copy in tile_sends(array, index, s):
            copy.start()

    def relay(array, index, s):
        copy = tile_pass(array, index, s)
        copy.wait_recv()
        copy.start()

    def complete(array, index, s):
        odd = lax.rem(s, 2)
        for slot in (beside * (1 - odd) + behind * odd, corner):
            place = array.at[slot, tile_rows(s)]
            remote(
                place, place, x_sem.at[index, s], slot_recv.at[index, slot, s], x_peer
            ).wait_recv()

    total_rows = tokens.shape[0]
    tiles = total_rows // TILE

    def loop(body):
        def run(s, carry):
            body(s)
            return carry

        lax.fori_loop(0, tiles, run, 0)

    def stage(index, array, work, earlier=None, before=None):
        def body(s):
            if before is not None:
                complete(before, index - 1, s)
            work(s)
            emit(array, index, s)
            if earlier is not None:
                pl.when(s == 0)(lambda: relay(earlier, index - 1, tiles - 1))
            pl.when(s > 0)(lambda: relay(array, index, s - 1))

        loop(body)

    def norm_rows(array, gain, s):
        width = array.shape[2]
        features = width * tp_size
        for piece in range(0, TILE, 64):
            rows = pl.ds(pl.multiple_of(s * TILE + piece, 64), 64)
            parts = [array[k, rows, :].astype(jnp.float32) for k in range(tp_size)]
            squares = sum(jnp.sum(part * part, axis=-1, keepdims=True) for part in parts)
            scale = lax.rsqrt(squares / features + EPSILON)
            for k, part in enumerate(parts):
                at = slice(k * width, (k + 1) * width)
                normed[rows, at] = (part * scale * gain[:, at]).astype(jnp.bfloat16)

    def dot(left, right):
        return jnp.dot(left, right, preferred_element_type=jnp.float32)

    def turned(rows, matrix):
        features = matrix.shape[1]
        width = matrix.shape[0] // fs_size
        return sum(
            lax.dot_general(
                normed[rows, k * features : (k + 1) * features],
                matrix[k * width : (k + 1) * width, :],
                (((1,), (1,)), ((), ())),
                preferred_element_type=jnp.float32,
            )
            for k in range(fs_size)
        )

    def gate_tile(matrix):
        def work(s):
            rows = tile_rows(s)
            gate_part[rows, :] = jax.nn.silu(turned(rows, matrix))

        return work

    def up_tile(matrix, hidden):
        def work(s):
            rows = tile_rows(s)
            product = gate_part[rows, :] * turned(rows, matrix)
            hidden[mine, rows, :] = product.astype(jnp.bfloat16)

        return work

    def lowered(hidden, down, residual, rows):
        width = hidden.shape[2]
        total = sum(
            dot(hidden[k, rows, :], down[k * width : (k + 1) * width, :]) for k in range(tp_size)
        )
        value = residual[mine, rows, :].astype(jnp.float32) + 0.5 * total
        return value.astype(jnp.bfloat16)

    def down_tile(s):
        rows = tile_rows(s)
        second[mine, rows, :] = lowered(hidden_one, whole[2], first, rows)

    def mix_tile(s):
        rows = tile_rows(s)
        norm_rows(second, mix_gain, s)
        width = channels.shape[2]
        products = dot(normed[rows, :], whole[3][...])
        channels[mine, rows, :] = mix_sequence(
            products[:, :width], products[:, width:], taps[...], gates[...], sharpness[...]
        )

    def out_tile(s):
        rows = tile_rows(s)
        norm_rows(channels, channel_gain, s)
        width = channels.shape[2] * tp_size
        total = dot(normed[rows, :width], whole[4][...])
        third[mine, rows, :] = (second[mine, rows, :].astype(jnp.float32) + total).astype(
            jnp.bfloat16
        )

    def out_send(s):
        rows = tile_rows(s)
        return remote(final.at[rows], out.at[rows], out_sem.at[s], out_recv.at[s], partner)

    count = len(shards)

    swap(0)
    keep_tokens = pltpu.make_async_copy(tokens, first.at[t], token_sem.at[0])
    when(home, keep_tokens.start)
    target, sem = first.at[t], token_recv.at[t]
    links.send(tokens, target, token_sem.at[1], sem, {"fs": across, "tp": 2 * y + x})
    links.send(tokens, target, token_sem.at[2], sem, {"tp": behind})
    links.send(tokens, target, token_sem.at[3], sem, twin, away)
    swap(1)
    settle(0)
    launch(0)
    launch_last(0)

    def token_arrive(slot, condition):
        place = first.at[slot]
        copy = remote(place, place, token_sem.at[1], token_recv.at[slot], y_peer)
        when(condition, copy.wait_recv)

    for k in range(2):
        slot = 2 * y + k
        token_arrive(slot, away)
        links.send(
            first.at[slot],
            first.at[slot],
            token_pass.at[k],
            token_recv.at[slot],
            y_peer,
            away,
        )
    for k, (own, target) in enumerate(zip(own_side, side)):
        links.send(own, target, side_sem.at[k], side_recv.at[k], partner, away)
        when(home, pltpu.make_async_copy(own, target, side_sem.at[k]).start)
    settle(1)
    launch(1)
    launch_last(1)
    for p in range(2, count):
        swap(p)
    when(home, keep_tokens.wait)
    token_arrive(other, home)
    token_arrive(2 * (1 - y), None)
    token_arrive(2 * (1 - y) + 1, None)
    loop(functools.partial(norm_rows, first, pre_gain))
    for p in range(2, 5):
        settle(p)
        launch(p)
    pump(0, inner)
    ready(0)
    loop(gate_tile(whole[0]))
    for p in range(5, count):
        settle(p)
        launch(p)
    pump(1, inner)
    launch_last(2)
    launch_last(3)
    ready(1)
    stage(1, hidden_one, up_tile(whole[1], hidden_one))
    pump(2, inner)
    relay(hidden_one, 1, tiles - 1)
    ready(2)
    stage(2, second, down_tile, before=hidden_one)
    pump(3, inner)
    launch_last(4)
    pump(4, inner)
    launch_last(5)
    for k, (own, target) in enumerate(zip(own_side, side)):
        when(home, pltpu.make_async_copy(own, target, side_sem.at[k]).wait)
        when(
            away, remote(own, target, side_sem.at[k], side_recv.at[k], partner).wait_recv
        )
    ready(3)
    stage(3, channels, mix_tile, earlier=second, before=second)
    pump(5, inner)
    launch_last(6)
    ready(4)
    stage(4, third, out_tile, earlier=channels, before=channels)
    relay(third, 4, tiles - 1)
    pump(6, inner)
    launch_last(7)
    ready(5)

    def post_gate_tile(s):
        complete(third, 4, s)
        norm_rows(third, post_gain, s)
        gate_tile(whole[5])(s)

    loop(post_gate_tile)
    pump(7, inner)
    ready(6)
    stage(5, hidden_two, up_tile(whole[6], hidden_two))
    relay(hidden_two, 5, tiles - 1)
    ready(7)

    def last_tile(s):
        rows = tile_rows(s)
        complete(hidden_two, 5, s)
        final[rows, :] = lowered(hidden_two, whole[7], third, rows)
        when(away, out_send(s).start)

        def keep():
            out[rows, :] = final[rows, :]

        when(home, keep)

    loop(last_tile)

    def drain_tiles(s):
        for index, array in enumerate((hidden_one, second, channels, third, hidden_two)):
            for copy in tile_sends(array, index + 1, s):
                copy.wait_send()
            tile_pass(array, index + 1, s).wait_send()
        when(away, out_send(s).wait_send)
        when(away, out_send(s).wait_recv)

    links.drain()
    loop(drain_tiles)


def fused(
    fs_size,
    tp_size,
    tokens,
    pre_gain,
    pre_gate,
    pre_up,
    pre_down,
    mix_gain,
    branch_proj,
    gate_proj,
    conv_taps,
    retain_blocks,
    admit_blocks,
    decay_param,
    channel_gain,
    out_proj,
    post_gain,
    post_gate,
    post_up,
    post_down,
):
    half_type = lambda array: array.astype(jnp.bfloat16)
    shards = [
        half_type(pre_gate.T),
        half_type(pre_up.T),
        half_type(pre_down),
        jnp.concatenate((half_type(branch_proj), half_type(gate_proj)), axis=1),
        half_type(out_proj),
        half_type(post_gate.T),
        half_type(post_up.T),
        half_type(post_down),
    ]
    gates = jnp.concatenate((spread_blocks(retain_blocks), spread_blocks(admit_blocks)), axis=1)
    sharpness = jax.nn.softplus(-decay_param)[None, :]
    rows, width = tokens.shape
    hidden = pre_gate.shape[1]
    operands = [
        tokens,
        pre_gain[None],
        mix_gain[None],
        channel_gain[None],
        post_gain[None],
        conv_taps,
        gates,
        sharpness,
        *shards,
    ]
    dma = pltpu.SemaphoreType.DMA
    count = len(shards)
    depth = fs_size // 2
    tiles = rows // TILE
    stacked = lambda columns: pltpu.VMEM((tp_size, rows, columns), jnp.bfloat16)
    return pl.pallas_call(
        functools.partial(layer_kernel, fs_size, tp_size),
        out_shape=jax.ShapeDtypeStruct(tokens.shape, tokens.dtype),
        in_specs=[pl.BlockSpec(memory_space=pltpu.VMEM)] * len(operands),
        out_specs=pl.BlockSpec(memory_space=pltpu.VMEM),
        scratch_shapes=[
            *(pltpu.VMEM((fs_size * s.shape[0], s.shape[1]), jnp.bfloat16) for s in shards),
            stacked(width),
            stacked(width),
            stacked(width),
            stacked(hidden),
            stacked(hidden),
            stacked(branch_proj.shape[1]),
            pltpu.VMEM((rows, width * tp_size), jnp.bfloat16),
            pltpu.VMEM((rows, hidden), jnp.float32),
            pltpu.VMEM((rows, width), jnp.bfloat16),
            *(pltpu.VMEM(s.shape, s.dtype) for s in (conv_taps, gates, sharpness)),
            dma((count, fs_size)),
            dma((count, depth)),
            dma((count, depth)),
            dma((count, 2)),
            dma((count, depth)),
            dma((count,)),
            dma((count,)),
            dma((4,)),
            dma((tp_size,)),
            dma((2,)),
            dma((6, tp_size, tiles)),
            dma((6, tiles)),
            dma((6, tiles)),
            dma((6, tiles)),
            dma((3,)),
            dma((3,)),
            dma((tiles,)),
            dma((tiles,)),
        ],
        compiler_params=pltpu.CompilerParams(
            collective_id=0, has_side_effects=True, vmem_limit_bytes=62 * 2**20
        ),
    )(*operands)


def fits_fused(fs_size, tp_size, arrays):
    shards = [a for i, a in enumerate(arrays) if i in (2, 3, 4, 6, 7, 13, 15, 16, 17)]
    rows_fit = all(a.shape[0] % 16 == 0 for a in shards)
    lanes_fit = all(arrays[i].shape[1] % 128 == 0 for i in (0, 6, 7))
    tiles_fit = arrays[0].shape[0] % TILE == 0 and arrays[2].shape[1] % 16 == 0
    turned_fit = all(arrays[i].shape[0] % 128 == 0 for i in (2, 3, 15, 16))
    return (
        rows_fit
        and lanes_fit
        and tiles_fit
        and turned_fit
        and fs_size % 2 == 0
        and 6 <= fs_size <= 16
        and tp_size == 4
    )


def local(
    tokens,
    pre_gain,
    pre_gate,
    pre_up,
    pre_down,
    mix_gain,
    branch_proj,
    gate_proj,
    conv_taps,
    retain_blocks,
    admit_blocks,
    decay_param,
    channel_gain,
    out_proj,
    post_gain,
    post_gate,
    post_up,
    post_down,
):
    after_pre = feed_forward(tokens, pre_gain, pre_gate, pre_up, pre_down)
    after_mix = recurrent_mixer(
        after_pre,
        mix_gain,
        branch_proj,
        gate_proj,
        conv_taps,
        retain_blocks,
        admit_blocks,
        decay_param,
        channel_gain,
        out_proj,
    )
    return feed_forward(after_mix, post_gain, post_gate, post_up, post_down)


def solution(mesh):
    placed = (
        P("fs", "tp"),
        P(),
        P("fs", "tp"),
        P("fs", "tp"),
        P("fs", "tp"),
        P(),
        P("fs", "tp"),
        P("fs", "tp"),
        P(None, "tp"),
        P("tp", None, None),
        P("tp", None, None),
        P("tp"),
        P(),
        P("fs", "tp"),
        P(),
        P("fs", "tp"),
        P("fs", "tp"),
        P("fs", "tp"),
    )
    fs_size, tp_size = mesh.shape["fs"], mesh.shape["tp"]

    def layer(*arrays):
        if fits_fused(fs_size, tp_size, arrays):
            return fused(fs_size, tp_size, *arrays)
        return local(*arrays)

    return jax.shard_map(
        layer, mesh=mesh, in_specs=placed, out_specs=P("fs", "tp"), check_vma=False
    )
```

```python
import functools

import jax
import jax.numpy as jnp
from jax import lax
from jax.experimental import pallas as pl
from jax.experimental.pallas import tpu as pltpu
from jax.sharding import PartitionSpec as P

SEQ_LEN = 128


EPSILON = 1e-06
DECAY_SCALE = 8.0


def normalize(values, norm_gain):
    floats = values.astype(jnp.float32)
    scaled = floats * lax.rsqrt(jnp.mean(floats * floats, axis=-1, keepdims=True) + EPSILON)
    return (scaled * norm_gain).astype(jnp.bfloat16)


def widen(residual):
    return lax.all_gather(residual, "tp", axis=1, tiled=True)


def contract(operand, stacked):
    return jnp.dot(
        operand,
        lax.all_gather(stacked.astype(jnp.bfloat16), "fs", axis=0, tiled=True),
        preferred_element_type=jnp.float32,
    )


def feed_forward(residual, norm_gain, gate_matrix, up_matrix, down_matrix):
    normed = normalize(widen(residual), norm_gain)
    products = contract(normed, jnp.concatenate((gate_matrix, up_matrix), axis=1))
    split_at = gate_matrix.shape[1]
    hidden = (jax.nn.silu(products[:, :split_at]) * products[:, split_at:]).astype(jnp.bfloat16)
    all_hidden = lax.all_gather(hidden, "tp", axis=1, tiled=True)
    return (residual.astype(jnp.float32) + 0.5 * contract(all_hidden, down_matrix)).astype(
        jnp.bfloat16
    )


def shifted(values, distance, fill):
    row = lax.broadcasted_iota(jnp.int32, values.shape, 0)
    return jnp.where(row >= distance, pltpu.roll(values, distance, 0), fill)


def mix_sequence(branch, gate_act, taps, gates, sharpness):
    width = branch.shape[1]
    count = taps.shape[0]
    convolved = branch * taps[count - 1 : count]
    for back in range(1, count):
        convolved = convolved + shifted(branch, back, 0.0) * taps[count - 1 - back : count - back]
    convolved = convolved.astype(jnp.bfloat16)
    both = jax.nn.sigmoid(jnp.dot(convolved, gates, preferred_element_type=jnp.float32))
    log_keep = -DECAY_SCALE * both[:, :width] * sharpness
    keep = jnp.exp(log_keep)
    inject = (
        jnp.sqrt(jnp.tanh(-log_keep) * (1.0 + keep * keep))
        * both[:, width:]
        * convolved.astype(jnp.float32)
    )
    distance = 1
    while distance < branch.shape[0]:
        inject = keep * shifted(inject, distance, 0.0) + inject
        keep = keep * shifted(keep, distance, 1.0)
        distance *= 2
    return (inject * jax.nn.gelu(gate_act)).astype(jnp.bfloat16)


def mix_kernel(products_ref, taps_ref, gates_ref, sharp_ref, out_ref):
    width = out_ref.shape[1]
    out_ref[...] = mix_sequence(
        products_ref[:, :width],
        products_ref[:, width:],
        taps_ref[...],
        gates_ref[...],
        sharp_ref[...],
    )


def spread_blocks(blocks):
    count, size, _ = blocks.shape
    eye = jnp.eye(count, dtype=blocks.dtype)
    wide = eye[:, None, :, None] * blocks[:, :, None, :]
    return wide.reshape(count * size, count * size).astype(jnp.bfloat16)


def recurrent_mixer(
    residual,
    norm_gain,
    branch_matrix,
    gate_matrix,
    conv_taps,
    retain_blocks,
    admit_blocks,
    decay_param,
    channel_gain,
    out_matrix,
):
    normed = normalize(widen(residual), norm_gain)
    products = contract(normed, jnp.concatenate((branch_matrix, gate_matrix), axis=1))
    width = branch_matrix.shape[1]
    rows = residual.shape[0]
    gates = jnp.concatenate((spread_blocks(retain_blocks), spread_blocks(admit_blocks)), axis=1)
    sharpness = jax.nn.softplus(-decay_param)[None, :]
    whole = lambda array: pl.BlockSpec(array.shape, lambda i: (0, 0))
    mixed_rows = pl.pallas_call(
        mix_kernel,
        grid=(rows // SEQ_LEN,),
        in_specs=[
            pl.BlockSpec((SEQ_LEN, 2 * width), lambda i: (i, 0)),
            whole(conv_taps),
            whole(gates),
            whole(sharpness),
        ],
        out_specs=pl.BlockSpec((SEQ_LEN, width), lambda i: (i, 0)),
        out_shape=jax.ShapeDtypeStruct((rows, width), jnp.bfloat16),
        cost_estimate=pl.CostEstimate(
            flops=rows * width * 1200, bytes_accessed=rows * width * 10, transcendentals=0
        ),
    )(products, conv_taps, gates, sharpness)
    all_channels = lax.all_gather(mixed_rows, "tp", axis=1, tiled=True)
    mixed_normed = normalize(all_channels, channel_gain)
    return (residual.astype(jnp.float32) + contract(mixed_normed, out_matrix)).astype(jnp.bfloat16)


TILE = SEQ_LEN
OUT_SPACE = pltpu.VMEM
MESH = pl.DeviceIdType.MESH


def when(condition, action):
    if condition is None:
        action()
    else:
        pl.when(condition)(action)


class Exchange:
    def __init__(self):
        self.sent = []

    def send(self, source, target, send_sem, recv_sem, device, condition=None):
        copy = remote(source, target, send_sem, recv_sem, device)
        when(condition, copy.start)
        self.sent.append((copy, condition))

    def drain(self):
        for copy, condition in self.sent:
            when(condition, copy.wait_send)


def remote(source, target, send_sem, recv_sem, device):
    return pltpu.make_async_remote_copy(
        src_ref=source,
        dst_ref=target,
        send_sem=send_sem,
        recv_sem=recv_sem,
        device_id=device,
        device_id_type=MESH,
    )


def softplus(values):
    return jnp.maximum(values, 0.0) + jnp.log1p(jnp.exp(-jnp.abs(values)))


def layer_kernel(fs_size, tp_size, *refs):
    (tokens, pre_gain, mix_gain, channel_gain, post_gain) = refs[:5]
    own_side = refs[5:9]
    matrices = refs[9:18]
    out = refs[18]
    refs = refs[19:]
    whole = refs[:8]
    shards = refs[8:16]
    raw = refs[16:25]
    first, second, third, channels = refs[25:29]
    hidden_one, hidden_two = refs[29:31], refs[31:33]
    normed, final, gates = refs[33:36]
    refs = refs[1:]
    side = refs[35:39]
    recv_sem, up_sem, down_sem, pair_sem, swap_sem, keep_sem, raw_sem = refs[39:46]
    token_sem, token_recv, token_pass = refs[46:49]
    slot_recv, x_sem, y_sem, pass_sem = refs[49:53]
    side_sem, side_recv, out_sem, out_recv = refs[53:57]
    taps, retain, admit, decay = side

    f = lax.axis_index("fs")
    t = lax.axis_index("tp")
    x = lax.rem(f, 2)
    z = f // 2
    y = t // 2
    c = lax.rem(t, 2)
    depth = fs_size // 2
    home = x == c
    away = x != c
    end = (z == 0) | (z == depth - 1)
    inner = (z > 0) & (z < depth - 1)

    mine = 2 * y + x
    beside = 2 * y + 1 - x
    behind = 2 * (1 - y) + x
    corner = 2 * (1 - y) + 1 - x
    line = 2 * z + c

    across = f + 1 - 2 * x
    other = t + 1 - 2 * c
    x_peer = {"fs": across}
    y_peer = {"tp": lax.rem(t + 2, tp_size)}
    twin = {"tp": other}
    partner = {"fs": across, "tp": other}
    skew = {"tp": lax.rem(other + 2, tp_size)}
    above = {"fs": lax.rem(f + 2, fs_size)}
    below = {"fs": lax.rem(f + fs_size - 2, fs_size)}
    links = Exchange()

    def load(m):
        return pltpu.make_async_copy(matrices[m], raw[m], raw_sem.at[m])

    for m in range(len(matrices)):
        load(m).start()

    def turn(source, halves, at):
        width = source.shape[1]
        half = width // 2
        for start in range(0, width, 128):
            stop = min(start + 128, width)
            piece = source[:, start:stop].T.astype(jnp.bfloat16)
            for k, target in enumerate(halves):
                low, high = max(start, k * half), min(stop, (k + 1) * half)
                if low < high:
                    to = at + low - k * half
                    target[to : to + high - low, :] = piece[low - start : high - start, :]

    def copy_in(source, target, at):
        target[:, at : at + source.shape[1]] = source[...].astype(jnp.bfloat16)

    def convert(p):
        parts = {0: (0, 1), 2: (2,), 3: (3, 4), 4: (5,), 5: (6, 7), 7: (8,)}.get(p, ())
        at = 0
        for m in parts:
            load(m).wait()
            if p in (0, 5):
                turn(raw[m], shards[p : p + 2], at)
                at += raw[m].shape[1] // 2
            else:
                copy_in(raw[m], shards[p], at)
                at += raw[m].shape[1]

    barrier = pltpu.get_barrier_semaphore()
    greeted = [
        (x_peer, None),
        (y_peer, None),
        (twin, None),
        (partner, None),
        (skew, None),
        (above, z < depth - 1),
        (below, z > 0),
    ]
    expected = 0
    for device, condition in greeted:
        when(
            condition,
            functools.partial(
                pl.semaphore_signal, barrier, inc=1, device_id=device, device_id_type=MESH
            ),
        )
        expected = expected + (1 if condition is None else condition.astype(jnp.int32))
    convert(0)
    pl.semaphore_wait(barrier, expected)

    def block(p, owner):
        rows = shards[p].shape[0]
        return whole[p].at[pl.ds(pl.multiple_of(owner * rows, rows), rows)]

    def arrive(p, owner, condition=None):
        place = block(p, owner)
        copy = remote(place, place, pair_sem.at[p, 0], recv_sem.at[p, owner], twin)
        when(condition, copy.wait_recv)

    def swap(p):
        links.send(
            shards[p], block(p, f), swap_sem.at[p], recv_sem.at[p, f], partner, away
        )
        when(home, pltpu.make_async_copy(shards[p], block(p, f), keep_sem.at[p]).start)

    def settle(p, who=None):
        if who is None or who == "home":
            when(home, pltpu.make_async_copy(shards[p], block(p, f), keep_sem.at[p]).wait)
        if who is None or who == "away":
            arrive(p, line, away)

    def launch(p, who):
        place, sem = block(p, line), recv_sem.at[p, line]
        links.send(place, place, up_sem.at[p, z], sem, above, who & (z < depth - 1))
        links.send(place, place, down_sem.at[p, z], sem, below, who & (z > 0))
        links.send(place, place, pair_sem.at[p, z], sem, twin, who)

    def take(p, level, condition):
        owner = 2 * level + c
        arrive(p, owner, condition)
        place, sem = block(p, owner), recv_sem.at[p, owner]
        upward = condition & (z < depth - 1) & (level < z)
        downward = condition & (z > 0) & (level > z)
        links.send(place, place, up_sem.at[p, level], sem, above, upward)
        links.send(place, place, down_sem.at[p, level], sem, below, downward)
        links.send(place, place, pair_sem.at[p, level], sem, twin, condition)

    def pump(p, condition):
        for distance in range(1, depth):
            for sign in (-1, 1):
                level = z + sign * distance
                exists = (level >= 0) & (level < depth)
                take(p, lax.rem(level + depth, depth), condition & exists)

    def ready(p):
        pump(p, end)
        for level in range(depth):
            if p == 0:
                arrive(p, 2 * level + 1 - c, away | (z != level))
            else:
                arrive(p, 2 * level + 1 - c)

    def tile_rows(s):
        return pl.ds(pl.multiple_of(s * TILE, TILE), TILE)

    def tile_sends(array, index, s):
        rows = tile_rows(s)
        place, sem = array.at[mine, rows], slot_recv.at[index, mine, s]
        return (
            remote(place, place, x_sem.at[index, s], sem, x_peer),
            remote(place, place, y_sem.at[index, s], sem, y_peer),
        )

    def tile_pass(array, index, s):
        odd = lax.rem(s, 2)
        slot = behind * (1 - odd) + beside * odd
        place = array.at[slot, tile_rows(s)]
        device = {
            "fs": f + (1 - odd) * (1 - 2 * x),
            "tp": lax.rem(t + 2 * odd, tp_size),
        }
        return remote(
            place, place, pass_sem.at[index, s], slot_recv.at[index, slot, s], device
        )

    def emit(array, index, s):
        for copy in tile_sends(array, index, s):
            copy.start()

    def relay(array, index, s):
        copy = tile_pass(array, index, s)
        copy.wait_recv()
        copy.start()

    def complete(array, index, s):
        odd = lax.rem(s, 2)
        for slot in (beside * (1 - odd) + behind * odd, corner):
            place = array.at[slot, tile_rows(s)]
            remote(
                place, place, x_sem.at[index, s], slot_recv.at[index, slot, s], x_peer
            ).wait_recv()

    total_rows = tokens.shape[0]
    tiles = total_rows // TILE

    def loop(body):
        def run(s, carry):
            body(s)
            return carry

        lax.fori_loop(0, tiles, run, 0)

    def stage(index, array, work, earlier=None, before=()):
        def body(s):
            for k, ready_array in before:
                complete(ready_array, k, s)
            work(s)
            emit(array, index, s)
            if earlier is not None:
                k, ready_array = earlier
                pl.when(s == 0)(lambda: relay(ready_array, k, tiles - 1))
            pl.when(s > 0)(lambda: relay(array, index, s - 1))

        loop(body)

    def norm_rows(array, gain, s):
        width = array.shape[2]
        features = width * tp_size
        for piece in range(0, TILE, 64):
            rows = pl.ds(pl.multiple_of(s * TILE + piece, 64), 64)
            parts = [array[k, rows, :].astype(jnp.float32) for k in range(tp_size)]
            squares = sum(jnp.sum(part * part, axis=-1, keepdims=True) for part in parts)
            scale = lax.rsqrt(squares / features + EPSILON)
            for k, part in enumerate(parts):
                at = slice(k * width, (k + 1) * width)
                normed[rows, at] = (part * scale * gain[:, at]).astype(jnp.bfloat16)

    def dot(left, right):
        return jnp.dot(left, right, preferred_element_type=jnp.float32)

    def turned(rows, matrix, part):
        features = matrix.shape[1]
        width = matrix.shape[0] // fs_size
        half = width // 2
        return sum(
            lax.dot_general(
                normed[rows, k * features : (k + 1) * features],
                matrix[k * width + part * half : k * width + (part + 1) * half, :],
                (((1,), (1,)), ((), ())),
                preferred_element_type=jnp.float32,
            )
            for k in range(fs_size)
        )

    def hidden_tile(matrix, hidden):
        def work(s):
            rows = tile_rows(s)
            product = jax.nn.silu(turned(rows, matrix, 0)) * turned(rows, matrix, 1)
            hidden[mine, rows, :] = product.astype(jnp.bfloat16)

        return work

    def lowered(halves, down, residual, rows):
        half = halves[0].shape[2]
        total = sum(
            dot(
                hidden[k, rows, :],
                down[(2 * k + part) * half : (2 * k + part + 1) * half, :],
            )
            for k in range(tp_size)
            for part, hidden in enumerate(halves)
        )
        value = residual[mine, rows, :].astype(jnp.float32) + 0.5 * total
        return value.astype(jnp.bfloat16)

    def down_tile(s):
        rows = tile_rows(s)
        second[mine, rows, :] = lowered(hidden_one, whole[2], first, rows)

    def mix_tile(s):
        rows = tile_rows(s)
        norm_rows(second, mix_gain, s)
        width = channels.shape[2]
        products = dot(normed[rows, :], whole[3][...])
        channels[mine, rows, :] = mix_sequence(
            products[:, :width], products[:, width:], taps[...], gates[...], softplus(-decay[...])
        )

    def out_tile(s):
        rows = tile_rows(s)
        norm_rows(channels, channel_gain, s)
        width = channels.shape[2] * tp_size
        total = dot(normed[rows, :width], whole[4][...])
        third[mine, rows, :] = (second[mine, rows, :].astype(jnp.float32) + total).astype(
            jnp.bfloat16
        )

    def out_send(s):
        rows = tile_rows(s)
        return remote(final.at[rows], out.at[rows], out_sem.at[s], out_recv.at[s], partner)

    def out_keep(s):
        rows = tile_rows(s)
        return pltpu.make_async_copy(final.at[rows], out.at[rows], out_sem.at[s])

    def spread(blocks, at):
        size = blocks.shape[1]
        for k in range(blocks.shape[0]):
            place = slice(k * size, (k + 1) * size)
            gates[place, at + k * size : at + (k + 1) * size] = blocks[k].astype(jnp.bfloat16)

    count = len(shards)
    gates[...] = jnp.zeros_like(gates)

    def token_arrive(slot, condition):
        place = first.at[slot]
        copy = remote(place, place, token_sem.at[1], token_recv.at[slot], y_peer)
        when(condition, copy.wait_recv)

    def token_cross(who):
        links.send(
            tokens,
            first.at[t],
            token_sem.at[1],
            token_recv.at[t],
            {"fs": across, "tp": 2 * y + x},
            who,
        )

    def side_copies():
        for k, (own, target) in enumerate(zip(own_side, side)):
            yield (
                remote(own, target, side_sem.at[k], side_recv.at[k], partner),
                pltpu.make_async_copy(own, target, side_sem.at[k]),
            )

    swap(0)
    keep_tokens = pltpu.make_async_copy(tokens, first.at[t], token_sem.at[0])
    when(home, keep_tokens.start)
    target, sem = first.at[t], token_recv.at[t]
    links.send(tokens, target, token_sem.at[2], sem, {"tp": behind})
    links.send(tokens, target, token_sem.at[3], sem, twin, away)
    settle(0, "home")
    launch(0, home)
    convert(1)
    swap(1)
    token_cross(away)
    settle(1, "home")
    launch(1, home)
    arrive(0, 2 * z + 1 - c, home)
    token_cross(home)
    settle(0, "away")
    launch(0, away)
    for p in range(2, count):
        convert(p)
        swap(p)
    for p in range(2, count):
        settle(p, "home")
        launch(p, home & end)
    pump(0, inner & home)
    settle(1, "away")
    launch(1, away)
    pump(0, inner & away)
    for k in range(2):
        slot = 2 * y + k
        token_arrive(slot, away)
        links.send(
            first.at[slot],
            first.at[slot],
            token_pass.at[k],
            token_recv.at[slot],
            y_peer,
            away,
        )
    for away_copy, home_copy in side_copies():
        when(away, away_copy.start)
        when(home, home_copy.start)
    when(home, keep_tokens.wait)
    token_arrive(other, home)
    token_arrive(2 * (1 - y), home)
    token_arrive(2 * (1 - y) + 1, home)
    pump(1, inner)
    for p in range(2, 4):
        settle(p, "away")
        launch(p, inner | away)
    token_arrive(2 * (1 - y), away)
    token_arrive(2 * (1 - y) + 1, away)
    loop(functools.partial(norm_rows, first, pre_gain))
    ready(0)
    stage(1, hidden_one[0], hidden_tile(whole[0], hidden_one[0]))
    for p in range(4, count):
        settle(p, "away")
        launch(p, away & end)
    pump(2, inner)
    launch(4, inner)
    relay(hidden_one[0], 1, tiles - 1)
    ready(1)
    stage(2, hidden_one[1], hidden_tile(whole[1], hidden_one[1]))
    pump(3, inner)
    launch(5, inner)
    relay(hidden_one[1], 2, tiles - 1)
    for away_copy, home_copy in side_copies():
        when(away, away_copy.wait)
        when(home, home_copy.wait)
    spread(retain, 0)
    spread(admit, gates.shape[0])
    ready(2)
    stage(3, second, down_tile, before=((1, hidden_one[0]), (2, hidden_one[1])))
    pump(4, inner)
    pump(5, inner)
    launch(6, inner)
    ready(3)
    stage(4, channels, mix_tile, earlier=(3, second), before=((3, second),))
    pump(6, inner)
    launch(7, inner)
    ready(4)
    stage(5, third, out_tile, earlier=(4, channels), before=((4, channels),))
    pump(7, inner)
    relay(third, 5, tiles - 1)
    ready(5)
    post_tile = hidden_tile(whole[5], hidden_two[0])

    def post_norm_tile(s):
        norm_rows(third, post_gain, s)
        post_tile(s)

    stage(6, hidden_two[0], post_norm_tile, before=((5, third),))
    relay(hidden_two[0], 6, tiles - 1)
    ready(6)
    stage(7, hidden_two[1], hidden_tile(whole[6], hidden_two[1]))
    relay(hidden_two[1], 7, tiles - 1)
    ready(7)

    def last_tile(s):
        rows = tile_rows(s)
        complete(hidden_two[0], 6, s)
        complete(hidden_two[1], 7, s)
        final[rows, :] = lowered(hidden_two, whole[7], third, rows)
        when(away, out_send(s).start)
        when(home, out_keep(s).start)

    loop(last_tile)
    gathered = (*hidden_one, second, channels, third, *hidden_two)

    def drain_tiles(s):
        for index, array in enumerate(gathered):
            for copy in tile_sends(array, index + 1, s):
                copy.wait_send()
            tile_pass(array, index + 1, s).wait_send()
        when(away, out_send(s).wait)
        when(home, out_keep(s).wait)

    links.drain()
    loop(drain_tiles)


def fused(
    fs_size,
    tp_size,
    tokens,
    pre_gain,
    pre_gate,
    pre_up,
    pre_down,
    mix_gain,
    branch_proj,
    gate_proj,
    conv_taps,
    retain_blocks,
    admit_blocks,
    decay_param,
    channel_gain,
    out_proj,
    post_gain,
    post_gate,
    post_up,
    post_down,
):
    matrices = [
        pre_gate,
        pre_up,
        pre_down,
        branch_proj,
        gate_proj,
        out_proj,
        post_gate,
        post_up,
        post_down,
    ]
    shards = [
        pre_gate.shape[::-1],
        pre_gate.shape[::-1],
        pre_down.shape,
        (branch_proj.shape[0], branch_proj.shape[1] + gate_proj.shape[1]),
        out_proj.shape,
        post_gate.shape[::-1],
        post_gate.shape[::-1],
        post_down.shape,
    ]
    rows, width = tokens.shape
    hidden = pre_gate.shape[1]
    channels = branch_proj.shape[1]
    side = [conv_taps, retain_blocks, admit_blocks, decay_param[None]]
    operands = [
        tokens,
        pre_gain[None],
        mix_gain[None],
        channel_gain[None],
        post_gain[None],
        *side,
        *matrices,
    ]
    dma = pltpu.SemaphoreType.DMA
    count = len(shards)
    depth = fs_size // 2
    tiles = rows // TILE
    stacked = lambda columns: pltpu.VMEM((tp_size, rows, columns), jnp.bfloat16)
    return pl.pallas_call(
        functools.partial(layer_kernel, fs_size, tp_size),
        out_shape=jax.ShapeDtypeStruct(tokens.shape, tokens.dtype),
        in_specs=[pl.BlockSpec(memory_space=pltpu.VMEM)] * (5 + len(side))
        + [pl.BlockSpec(memory_space=pl.ANY)] * len(matrices),
        out_specs=pl.BlockSpec(memory_space=OUT_SPACE),
        scratch_shapes=[
            *(pltpu.VMEM((fs_size * s[0], s[1]), jnp.bfloat16) for s in shards),
            *(pltpu.VMEM(s, jnp.bfloat16) for s in shards),
            *(pltpu.VMEM(m.shape, m.dtype) for m in matrices),
            stacked(width),
            stacked(width),
            stacked(width),
            stacked(channels),
            stacked(hidden // 2),
            stacked(hidden // 2),
            stacked(hidden // 2),
            stacked(hidden // 2),
            pltpu.VMEM((rows, width * tp_size), jnp.bfloat16),
            pltpu.VMEM((rows, width), jnp.bfloat16),
            pltpu.VMEM((channels, 2 * channels), jnp.bfloat16),
            *(pltpu.VMEM(s.shape, s.dtype) for s in side),
            dma((count, fs_size)),
            dma((count, depth)),
            dma((count, depth)),
            dma((count, depth)),
            dma((count,)),
            dma((count,)),
            dma((len(matrices),)),
            dma((4,)),
            dma((tp_size,)),
            dma((2,)),
            dma((8, tp_size, tiles)),
            dma((8, tiles)),
            dma((8, tiles)),
            dma((8, tiles)),
            dma((len(side),)),
            dma((len(side),)),
            dma((tiles,)),
            dma((tiles,)),
        ],
        compiler_params=pltpu.CompilerParams(
            collective_id=0, has_side_effects=True, vmem_limit_bytes=62 * 2**20
        ),
    )(*operands)


def fits_fused(fs_size, tp_size, arrays):
    shards = [a for i, a in enumerate(arrays) if i in (2, 3, 4, 6, 7, 13, 15, 16, 17)]
    rows_fit = all(a.shape[0] % 16 == 0 for a in shards)
    lanes_fit = all(arrays[i].shape[1] % 128 == 0 for i in (0, 6, 7))
    tiles_fit = arrays[0].shape[0] % TILE == 0 and arrays[2].shape[1] % 32 == 0
    turned_fit = all(arrays[i].shape[0] % 128 == 0 for i in (2, 3, 15, 16))
    return (
        rows_fit
        and lanes_fit
        and tiles_fit
        and turned_fit
        and fs_size % 2 == 0
        and 6 <= fs_size <= 16
        and tp_size == 4
    )


def local(
    tokens,
    pre_gain,
    pre_gate,
    pre_up,
    pre_down,
    mix_gain,
    branch_proj,
    gate_proj,
    conv_taps,
    retain_blocks,
    admit_blocks,
    decay_param,
    channel_gain,
    out_proj,
    post_gain,
    post_gate,
    post_up,
    post_down,
):
    after_pre = feed_forward(tokens, pre_gain, pre_gate, pre_up, pre_down)
    after_mix = recurrent_mixer(
        after_pre,
        mix_gain,
        branch_proj,
        gate_proj,
        conv_taps,
        retain_blocks,
        admit_blocks,
        decay_param,
        channel_gain,
        out_proj,
    )
    return feed_forward(after_mix, post_gain, post_gate, post_up, post_down)


def solution(mesh):
    placed = (
        P("fs", "tp"),
        P(),
        P("fs", "tp"),
        P("fs", "tp"),
        P("fs", "tp"),
        P(),
        P("fs", "tp"),
        P("fs", "tp"),
        P(None, "tp"),
        P("tp", None, None),
        P("tp", None, None),
        P("tp"),
        P(),
        P("fs", "tp"),
        P(),
        P("fs", "tp"),
        P("fs", "tp"),
        P("fs", "tp"),
    )
    fs_size, tp_size = mesh.shape["fs"], mesh.shape["tp"]

    def layer(*arrays):
        if fits_fused(fs_size, tp_size, arrays):
            return fused(fs_size, tp_size, *arrays)
        return local(*arrays)

    return jax.shard_map(
        layer, mesh=mesh, in_specs=placed, out_specs=P("fs", "tp"), check_vma=False
    )
```

```python
import functools

import jax
import jax.numpy as jnp
from jax import lax
from jax.experimental import pallas as pl
from jax.experimental.pallas import tpu as pltpu
from jax.sharding import PartitionSpec as P

SEQ_LEN = 128


EPSILON = 1e-06
DECAY_SCALE = 8.0


def normalize(values, norm_gain):
    floats = values.astype(jnp.float32)
    scaled = floats * lax.rsqrt(jnp.mean(floats * floats, axis=-1, keepdims=True) + EPSILON)
    return (scaled * norm_gain).astype(jnp.bfloat16)


def widen(residual):
    return lax.all_gather(residual, "tp", axis=1, tiled=True)


def contract(operand, stacked):
    return jnp.dot(
        operand,
        lax.all_gather(stacked.astype(jnp.bfloat16), "fs", axis=0, tiled=True),
        preferred_element_type=jnp.float32,
    )


def feed_forward(residual, norm_gain, gate_matrix, up_matrix, down_matrix):
    normed = normalize(widen(residual), norm_gain)
    products = contract(normed, jnp.concatenate((gate_matrix, up_matrix), axis=1))
    split_at = gate_matrix.shape[1]
    hidden = (jax.nn.silu(products[:, :split_at]) * products[:, split_at:]).astype(jnp.bfloat16)
    all_hidden = lax.all_gather(hidden, "tp", axis=1, tiled=True)
    return (residual.astype(jnp.float32) + 0.5 * contract(all_hidden, down_matrix)).astype(
        jnp.bfloat16
    )


def shifted(values, distance, fill):
    row = lax.broadcasted_iota(jnp.int32, values.shape, 0)
    return jnp.where(row >= distance, pltpu.roll(values, distance, 0), fill)


def mix_sequence(branch, gate_act, taps, gates, sharpness):
    width = branch.shape[1]
    count = taps.shape[0]
    convolved = branch * taps[count - 1 : count]
    for back in range(1, count):
        convolved = convolved + shifted(branch, back, 0.0) * taps[count - 1 - back : count - back]
    convolved = convolved.astype(jnp.bfloat16)
    both = jax.nn.sigmoid(jnp.dot(convolved, gates, preferred_element_type=jnp.float32))
    log_keep = -DECAY_SCALE * both[:, :width] * sharpness
    keep = jnp.exp(log_keep)
    inject = (
        jnp.sqrt(jnp.tanh(-log_keep) * (1.0 + keep * keep))
        * both[:, width:]
        * convolved.astype(jnp.float32)
    )
    distance = 1
    while distance < branch.shape[0]:
        inject = keep * shifted(inject, distance, 0.0) + inject
        keep = keep * shifted(keep, distance, 1.0)
        distance *= 2
    return (inject * jax.nn.gelu(gate_act)).astype(jnp.bfloat16)


def mix_kernel(products_ref, taps_ref, gates_ref, sharp_ref, out_ref):
    width = out_ref.shape[1]
    out_ref[...] = mix_sequence(
        products_ref[:, :width],
        products_ref[:, width:],
        taps_ref[...],
        gates_ref[...],
        sharp_ref[...],
    )


def spread_blocks(blocks):
    count, size, _ = blocks.shape
    eye = jnp.eye(count, dtype=blocks.dtype)
    wide = eye[:, None, :, None] * blocks[:, :, None, :]
    return wide.reshape(count * size, count * size).astype(jnp.bfloat16)


def recurrent_mixer(
    residual,
    norm_gain,
    branch_matrix,
    gate_matrix,
    conv_taps,
    retain_blocks,
    admit_blocks,
    decay_param,
    channel_gain,
    out_matrix,
):
    normed = normalize(widen(residual), norm_gain)
    products = contract(normed, jnp.concatenate((branch_matrix, gate_matrix), axis=1))
    width = branch_matrix.shape[1]
    rows = residual.shape[0]
    gates = jnp.concatenate((spread_blocks(retain_blocks), spread_blocks(admit_blocks)), axis=1)
    sharpness = jax.nn.softplus(-decay_param)[None, :]
    whole = lambda array: pl.BlockSpec(array.shape, lambda i: (0, 0))
    mixed_rows = pl.pallas_call(
        mix_kernel,
        grid=(rows // SEQ_LEN,),
        in_specs=[
            pl.BlockSpec((SEQ_LEN, 2 * width), lambda i: (i, 0)),
            whole(conv_taps),
            whole(gates),
            whole(sharpness),
        ],
        out_specs=pl.BlockSpec((SEQ_LEN, width), lambda i: (i, 0)),
        out_shape=jax.ShapeDtypeStruct((rows, width), jnp.bfloat16),
        cost_estimate=pl.CostEstimate(
            flops=rows * width * 1200, bytes_accessed=rows * width * 10, transcendentals=0
        ),
    )(products, conv_taps, gates, sharpness)
    all_channels = lax.all_gather(mixed_rows, "tp", axis=1, tiled=True)
    mixed_normed = normalize(all_channels, channel_gain)
    return (residual.astype(jnp.float32) + contract(mixed_normed, out_matrix)).astype(jnp.bfloat16)


TILE = SEQ_LEN
TAKEN = 3
MESH = pl.DeviceIdType.MESH


def when(condition, action):
    if condition is None:
        action()
    else:
        pl.when(condition)(action)


class Exchange:
    def __init__(self):
        self.sent = []

    def send(self, source, target, send_sem, recv_sem, device, condition=None):
        copy = remote(source, target, send_sem, recv_sem, device)
        when(condition, copy.start)
        self.sent.append((copy, condition))

    def drain(self):
        for copy, condition in self.sent:
            when(condition, copy.wait_send)


def remote(source, target, send_sem, recv_sem, device):
    return pltpu.make_async_remote_copy(
        src_ref=source,
        dst_ref=target,
        send_sem=send_sem,
        recv_sem=recv_sem,
        device_id=device,
        device_id_type=MESH,
    )


def softplus(values):
    return jnp.maximum(values, 0.0) + jnp.log1p(jnp.exp(-jnp.abs(values)))


def layer_kernel(fs_size, tp_size, *refs):
    (tokens, pre_gain, mix_gain, channel_gain, post_gain) = refs[:5]
    own_side = refs[5:9]
    matrices = refs[9:18]
    out = refs[18]
    refs = refs[19:]
    whole = refs[:9]
    shards = refs[9:18]
    raw = refs[18:27]
    refs = refs[2:]
    first, second, third, channels = refs[25:29]
    hidden_one, hidden_two = refs[29:31], refs[31:33]
    normed, final, gates = refs[33:36]
    refs = refs[1:]
    side = refs[35:39]
    recv_sem, twin_sem, pace_sem, own_sem, take_sem, swap_sem, raw_sem = refs[39:46]
    token_sem, token_recv, token_pass = refs[46:49]
    slot_recv, slot_sem = refs[49:51]
    side_sem, side_recv, out_sem, out_recv = refs[51:55]
    taps, retain, admit, decay = side

    f = lax.axis_index("fs")
    t = lax.axis_index("tp")
    x = lax.rem(f, 2)
    z = f // 2
    y = t // 2
    c = lax.rem(t, 2)
    depth = fs_size // 2
    home = x == c
    away = x != c
    end = (z == 0) | (z == depth - 1)
    inner = (z > 0) & (z < depth - 1)

    mine = 2 * y + x
    beside = 2 * y + 1 - x
    behind = 2 * (1 - y) + x
    corner = 2 * (1 - y) + 1 - x
    line = 2 * z + c

    across = f + 1 - 2 * x
    other = t + 1 - 2 * c
    x_peer = {"fs": across}
    y_peer = {"tp": lax.rem(t + 2, tp_size)}
    twin = {"tp": other}
    partner = {"fs": across, "tp": other}
    skew = {"tp": lax.rem(other + 2, tp_size)}
    above = {"fs": lax.rem(f + 2, fs_size)}
    below = {"fs": lax.rem(f + fs_size - 2, fs_size)}
    links = Exchange()

    def load(m):
        return pltpu.make_async_copy(matrices[m], raw[m], raw_sem.at[m])

    for m in range(len(matrices)):
        load(m).start()

    def convert(p):
        parts = {0: (0, 1), 2: (2,), 3: (3, 4), 4: (5,), 5: (6, 7), 7: (8,)}.get(p, ())
        at = 0
        for m in parts:
            load(m).wait()
            if p in (0, 5):
                half = raw[m].shape[0] // 2
                for k in range(2):
                    shards[p + k][at : at + half, :] = raw[m][
                        k * half : (k + 1) * half, :
                    ].astype(jnp.bfloat16)
                at += half
            elif p == 7:
                cut = shards[7].shape[1]
                shards[7][...] = raw[m][:, :cut].astype(jnp.bfloat16)
                shards[8][...] = raw[m][:, cut:].astype(jnp.bfloat16)
            else:
                shards[p][:, at : at + raw[m].shape[1]] = raw[m][...].astype(jnp.bfloat16)
                at += raw[m].shape[1]

    barrier = pltpu.get_barrier_semaphore()
    greeted = [
        (x_peer, None),
        (y_peer, None),
        (twin, None),
        (partner, None),
        (skew, None),
        (above, z < depth - 1),
        (below, z > 0),
    ]
    expected = 0
    for device, condition in greeted:
        when(
            condition,
            functools.partial(
                pl.semaphore_signal, barrier, inc=1, device_id=device, device_id_type=MESH
            ),
        )
        expected = expected + (1 if condition is None else condition.astype(jnp.int32))
    convert(0)
    pl.semaphore_wait(barrier, expected)

    def block(p, owner):
        rows = shards[p].shape[0]
        return whole[p].at[pl.ds(pl.multiple_of(owner * rows, rows), rows)]

    def arrive(p, level, condition=None):
        place = block(p, 2 * level + c)
        copy = remote(place, place, own_sem.at[p, 0], recv_sem.at[p, level], twin)
        when(condition, copy.wait_recv)

    def arrive_twin(p, blocks, sem, condition=None):
        place = whole[p].at[pl.ds(0, blocks * shards[p].shape[0])]
        copy = remote(place, place, own_sem.at[p, 0], sem, twin)
        when(condition, copy.wait_recv)

    def swap(p):
        links.send(shards[p], block(p, f), swap_sem.at[p], recv_sem.at[p, z], partner, away)
        when(home, pltpu.make_async_copy(shards[p], block(p, f), swap_sem.at[p]).start)

    def settle(p, who=None):
        if who is None or who == "home":
            when(home, pltpu.make_async_copy(shards[p], block(p, f), swap_sem.at[p]).wait)
        if who is None or who == "away":
            arrive(p, z, away)

    def launch(p, who):
        place, sem = block(p, line), recv_sem.at[p, z]
        links.send(place, place, own_sem.at[p, 1], sem, above, who & (z < depth - 2))
        links.send(place, place, own_sem.at[p, 2], sem, below, who & (z > 1))
        sem = pace_sem if p == 0 else twin_sem.at[p]
        links.send(place, place, own_sem.at[p, 0], sem, twin, who)

    def launch_last(p, who):
        place, sem = block(p, line), recv_sem.at[p, z]
        links.send(place, place, own_sem.at[p, 1], sem, above, who & (z == depth - 2))
        links.send(place, place, own_sem.at[p, 2], sem, below, who & (z == 1))

    taken = {}

    def take(p, key, level, condition):
        for copy, earlier in taken.get((p - TAKEN, key), ()):
            when(condition & earlier, copy.wait_send)
        arrive(p, level, condition)
        place = block(p, 2 * level + c)
        sends = (
            (recv_sem.at[p, level], above, condition & (z < depth - 1) & (level < z)),
            (recv_sem.at[p, level], below, condition & (z > 0) & (level > z)),
            (twin_sem.at[p], twin, condition),
        )
        for k, (sem, device, who) in enumerate(sends):
            copy = remote(place, place, take_sem.at[p % TAKEN, k, level], sem, device)
            when(who, copy.start)
            taken.setdefault((p, key), []).append((copy, who))

    def pump(p, condition):
        for distance in range(1, depth):
            for sign in (-1, 1):
                level = z + sign * distance
                exists = (level >= 0) & (level < depth)
                take(p, sign * distance, lax.rem(level + depth, depth), condition & exists)

    def ready(p):
        pump(p, end)
        if p == 0:
            arrive_twin(p, 1, pace_sem, away)
            arrive_twin(p, depth - 1, twin_sem.at[p])
        else:
            arrive_twin(p, depth, twin_sem.at[p])

    def tile_rows(s):
        return pl.ds(pl.multiple_of(s * TILE, TILE), TILE)

    def tile_sends(array, index, s):
        odd = lax.rem(s, 2)
        place = array.at[mine, tile_rows(s)]
        return (
            remote(
                place, place, slot_sem.at[0, s], slot_recv.at[index, 1 - odd, s], x_peer
            ),
            remote(place, place, slot_sem.at[1, s], slot_recv.at[index, odd, s], y_peer),
        )

    def tile_pass(array, index, s, kind):
        odd = lax.rem(s, 2)
        slot = behind * (1 - odd) + beside * odd
        place = array.at[slot, tile_rows(s)]
        device = {
            "fs": f + (1 - odd) * (1 - 2 * x),
            "tp": lax.rem(t + 2 * odd, tp_size),
        }
        return remote(place, place, slot_sem.at[2, s], slot_recv.at[index, kind, s], device)

    gathered = (None, *hidden_one, second, channels, third, *hidden_two)

    def emit(array, index, s):
        if index > 1:
            for copy in tile_sends(gathered[index - 1], index - 1, s):
                copy.wait_send()
        for copy in tile_sends(array, index, s):
            copy.start()

    def relay(array, index, s):
        if index > 1:
            tile_pass(gathered[index - 1], index - 1, s, 1).wait_send()
        tile_pass(array, index, s, 0).wait_recv()
        tile_pass(array, index, s, 1).start()

    def complete(array, index, s):
        place = array.at[pl.ds(0, 2), tile_rows(s)]
        remote(
            place, place, slot_sem.at[0, s], slot_recv.at[index, 1, s], x_peer
        ).wait_recv()

    total_rows = tokens.shape[0]
    tiles = total_rows // TILE

    def loop(body):
        def run(s, carry):
            body(s)
            return carry

        lax.fori_loop(0, tiles, run, 0)

    def stage(index, array, work, earlier=None, before=()):
        def body(s):
            for k, ready_array in before:
                complete(ready_array, k, s)
            work(s)
            emit(array, index, s)
            if earlier is not None:
                k, ready_array = earlier
                pl.when(s == 0)(lambda: relay(ready_array, k, tiles - 1))
            pl.when(s > 0)(lambda: relay(array, index, s - 1))

        loop(body)

    def norm_rows(array, gain, s):
        width = array.shape[2]
        features = width * tp_size
        for piece in range(0, TILE, 64):
            rows = pl.ds(pl.multiple_of(s * TILE + piece, 64), 64)
            parts = [array[k, rows, :].astype(jnp.float32) for k in range(tp_size)]
            squares = sum(jnp.sum(part * part, axis=-1, keepdims=True) for part in parts)
            scale = lax.rsqrt(squares / features + EPSILON)
            for k, part in enumerate(parts):
                at = slice(k * width, (k + 1) * width)
                normed[rows, at] = (part * scale * gain[:, at]).astype(jnp.bfloat16)

    def dot(left, right):
        return jnp.dot(left, right, preferred_element_type=jnp.float32)

    def turned(rows, matrix, part):
        features = matrix.shape[1]
        width = matrix.shape[0] // fs_size
        half = width // 2
        return sum(
            lax.dot_general(
                normed[rows, k * features : (k + 1) * features],
                matrix[k * width + part * half : k * width + (part + 1) * half, :],
                (((1,), (1,)), ((), ())),
                preferred_element_type=jnp.float32,
            )
            for k in range(fs_size)
        )

    def hidden_tile(matrix, hidden):
        def work(s):
            rows = tile_rows(s)
            product = jax.nn.silu(turned(rows, matrix, 0)) * turned(rows, matrix, 1)
            hidden[mine, rows, :] = product.astype(jnp.bfloat16)

        return work

    def lowered(halves, down, residual, rows, columns):
        half = halves[0].shape[2]
        total = sum(
            dot(
                hidden[k, rows, :],
                down[(2 * k + part) * half : (2 * k + part + 1) * half, :],
            )
            for k in range(tp_size)
            for part, hidden in enumerate(halves)
        )
        value = residual[mine, rows, columns].astype(jnp.float32) + 0.5 * total
        return value.astype(jnp.bfloat16)

    def down_tile(s):
        rows = tile_rows(s)
        second[mine, rows, :] = lowered(
            hidden_one, whole[2], first, rows, slice(None)
        )

    def mix_tile(s):
        rows = tile_rows(s)
        norm_rows(second, mix_gain, s)
        width = channels.shape[2]
        products = dot(normed[rows, :], whole[3][...])
        channels[mine, rows, :] = mix_sequence(
            products[:, :width], products[:, width:], taps[...], gates[...], softplus(-decay[...])
        )

    def out_tile(s):
        rows = tile_rows(s)
        norm_rows(channels, channel_gain, s)
        width = channels.shape[2] * tp_size
        total = dot(normed[rows, :width], whole[4][...])
        third[mine, rows, :] = (second[mine, rows, :].astype(jnp.float32) + total).astype(
            jnp.bfloat16
        )

    cut = shards[7].shape[1]
    last_columns = (slice(0, cut), slice(cut, cut + shards[8].shape[1]))

    def out_send(part, rows):
        place = (rows, last_columns[part])
        return remote(
            final.at[place], out.at[place], out_sem.at[part], out_recv.at[part], partner
        )

    def out_keep(part, rows):
        place = (rows, last_columns[part])
        return pltpu.make_async_copy(final.at[place], out.at[place], out_sem.at[part])

    def spread(blocks, at):
        size = blocks.shape[1]
        for k in range(blocks.shape[0]):
            place = slice(k * size, (k + 1) * size)
            gates[place, at + k * size : at + (k + 1) * size] = blocks[k].astype(jnp.bfloat16)

    count = len(shards)
    gates[...] = jnp.zeros_like(gates)

    def token_arrive(slot, condition):
        place = first.at[slot]
        copy = remote(place, place, token_sem.at[1], token_recv.at[slot], y_peer)
        when(condition, copy.wait_recv)

    def token_cross(who):
        links.send(
            tokens,
            first.at[t],
            token_sem.at[1],
            token_recv.at[t],
            {"fs": across, "tp": 2 * y + x},
            who,
        )

    def side_copies():
        for k, (own, target) in enumerate(zip(own_side, side)):
            yield (
                remote(own, target, side_sem.at[k], side_recv.at[k], partner),
                pltpu.make_async_copy(own, target, side_sem.at[k]),
            )

    swap(0)
    keep_tokens = pltpu.make_async_copy(tokens, first.at[t], token_sem.at[0])
    when(home, keep_tokens.start)
    target, sem = first.at[t], token_recv.at[t]
    links.send(tokens, target, token_sem.at[2], sem, {"tp": behind})
    links.send(tokens, target, token_sem.at[3], sem, twin, away)
    settle(0, "home")
    launch(0, home)
    launch_last(0, home)
    convert(1)
    swap(1)
    token_cross(away)
    settle(1, "home")
    launch_last(1, home)
    launch(1, home & end)
    arrive_twin(0, 1, pace_sem, home)
    token_cross(home)
    settle(0, "away")
    launch(0, away)
    launch_last(0, away)
    pump(0, inner & home)
    launch(1, home & inner)
    for p in range(2, count):
        convert(p)
        swap(p)
    for p in range(2, count):
        settle(p, "home")
    launch(2, home & inner)
    settle(1, "away")
    launch_last(1, away)
    launch(1, away & end)
    pump(0, inner & away)
    launch(1, away & inner)
    for k in range(2):
        slot = 2 * y + k
        token_arrive(slot, away)
        links.send(
            first.at[slot],
            first.at[slot],
            token_pass.at[k],
            token_recv.at[slot],
            y_peer,
            away,
        )
    for away_copy, home_copy in side_copies():
        when(away, away_copy.start)
        when(home, home_copy.start)
    when(home, keep_tokens.wait)
    token_arrive(other, home)
    token_arrive(2 * (1 - y), home)
    token_arrive(2 * (1 - y) + 1, home)
    for p in range(2, count):
        launch(p, home & end)
    pump(1, inner)
    for p in range(2, 4):
        settle(p, "away")
        launch(p, away)
    launch(3, home & inner)
    launch_last(2, inner)
    launch_last(3, inner)
    token_arrive(2 * (1 - y), away)
    token_arrive(2 * (1 - y) + 1, away)
    loop(functools.partial(norm_rows, first, pre_gain))
    ready(0)
    stage(1, hidden_one[0], hidden_tile(whole[0], hidden_one[0]))
    for p in range(4, count):
        settle(p, "away")
        launch(p, away & end)
    pump(2, inner)
    launch(4, inner)
    launch_last(4, inner)
    launch(5, inner)
    relay(hidden_one[0], 1, tiles - 1)
    ready(1)
    stage(2, hidden_one[1], hidden_tile(whole[1], hidden_one[1]))
    pump(3, inner)
    launch_last(5, inner)
    launch(6, inner)
    relay(hidden_one[1], 2, tiles - 1)
    for away_copy, home_copy in side_copies():
        when(away, away_copy.wait)
        when(home, home_copy.wait)
    spread(retain, 0)
    spread(admit, gates.shape[0])
    ready(2)
    stage(3, second, down_tile, before=((1, hidden_one[0]), (2, hidden_one[1])))
    pump(4, inner)
    pump(5, inner)
    launch_last(6, inner)
    launch(7, inner)
    launch(8, inner)
    ready(3)
    stage(4, channels, mix_tile, earlier=(3, second), before=((3, second),))
    pump(6, inner)
    launch_last(7, inner)
    launch_last(8, inner)
    ready(4)
    stage(5, third, out_tile, earlier=(4, channels), before=((4, channels),))
    pump(7, inner)
    pump(8, inner)
    relay(third, 5, tiles - 1)
    ready(5)
    post_tile = hidden_tile(whole[5], hidden_two[0])

    def post_norm_tile(s):
        norm_rows(third, post_gain, s)
        post_tile(s)

    stage(6, hidden_two[0], post_norm_tile, before=((5, third),))
    relay(hidden_two[0], 6, tiles - 1)
    ready(6)
    stage(7, hidden_two[1], hidden_tile(whole[6], hidden_two[1]))
    relay(hidden_two[1], 7, tiles - 1)
    for part, size in enumerate((2 * TILE, total_rows)):
        ready(7 + part)

        def last_rows(i, part=part, size=size):
            rows = pl.ds(pl.multiple_of(i * size, size), size)
            if part == 0:
                for k in range(2):
                    complete(hidden_two[0], 6, 2 * i + k)
                    complete(hidden_two[1], 7, 2 * i + k)
            final[rows, last_columns[part]] = lowered(
                hidden_two, whole[7 + part], third, rows, last_columns[part]
            )
            when(away, out_send(part, rows).start)
            when(home, out_keep(part, rows).start)

        if size == total_rows:
            last_rows(0)
        else:
            lax.fori_loop(0, total_rows // size, lambda i, carry: (last_rows(i), carry)[1], 0)

    links.drain()
    for (p, _), entries in taken.items():
        for copy, condition in entries if p >= count - TAKEN else ():
            when(condition, copy.wait_send)

    def drain_tiles(s):
        for copy in tile_sends(gathered[-1], len(gathered) - 1, s):
            copy.wait_send()
        tile_pass(gathered[-1], len(gathered) - 1, s, 1).wait_send()

    loop(drain_tiles)
    everything = pl.ds(0, total_rows)
    for part in range(2):
        when(away, out_send(part, everything).wait)
        when(home, out_keep(part, everything).wait)


def fused(
    fs_size,
    tp_size,
    tokens,
    pre_gain,
    pre_gate,
    pre_up,
    pre_down,
    mix_gain,
    branch_proj,
    gate_proj,
    conv_taps,
    retain_blocks,
    admit_blocks,
    decay_param,
    channel_gain,
    out_proj,
    post_gain,
    post_gate,
    post_up,
    post_down,
):
    matrices = [
        pre_gate.T,
        pre_up.T,
        pre_down,
        branch_proj,
        gate_proj,
        out_proj,
        post_gate.T,
        post_up.T,
        post_down,
    ]
    last = post_down.shape[1] - 128
    shards = [
        pre_gate.shape[::-1],
        pre_gate.shape[::-1],
        pre_down.shape,
        (branch_proj.shape[0], branch_proj.shape[1] + gate_proj.shape[1]),
        out_proj.shape,
        post_gate.shape[::-1],
        post_gate.shape[::-1],
        (post_down.shape[0], last),
        (post_down.shape[0], 128),
    ]
    rows, width = tokens.shape
    hidden = pre_gate.shape[1]
    channels = branch_proj.shape[1]
    side = [conv_taps, retain_blocks, admit_blocks, decay_param[None]]
    operands = [
        tokens,
        pre_gain[None],
        mix_gain[None],
        channel_gain[None],
        post_gain[None],
        *side,
        *matrices,
    ]
    dma = pltpu.SemaphoreType.DMA
    count = len(shards)
    depth = fs_size // 2
    tiles = rows // TILE
    stacked = lambda columns: pltpu.VMEM((tp_size, rows, columns), jnp.bfloat16)
    return pl.pallas_call(
        functools.partial(layer_kernel, fs_size, tp_size),
        out_shape=jax.ShapeDtypeStruct(tokens.shape, tokens.dtype),
        in_specs=[pl.BlockSpec(memory_space=pltpu.VMEM)] * (5 + len(side))
        + [pl.BlockSpec(memory_space=pl.ANY)] * len(matrices),
        out_specs=pl.BlockSpec(memory_space=pl.ANY),
        scratch_shapes=[
            *(pltpu.VMEM((fs_size * s[0], s[1]), jnp.bfloat16) for s in shards),
            *(pltpu.VMEM(s, jnp.bfloat16) for s in shards),
            *(pltpu.VMEM(m.shape, m.dtype) for m in matrices),
            stacked(width),
            stacked(width),
            stacked(width),
            stacked(channels),
            stacked(hidden // 2),
            stacked(hidden // 2),
            stacked(hidden // 2),
            stacked(hidden // 2),
            pltpu.VMEM((rows, width * tp_size), jnp.bfloat16),
            pltpu.VMEM((rows, width), jnp.bfloat16),
            pltpu.VMEM((channels, 2 * channels), jnp.bfloat16),
            *(pltpu.VMEM(s.shape, s.dtype) for s in side),
            dma((count, depth)),
            dma((count,)),
            dma,
            dma((count, 3)),
            dma((TAKEN, 3, depth)),
            dma((count,)),
            dma((len(matrices),)),
            dma((4,)),
            dma((tp_size,)),
            dma((2,)),
            dma((8, 2, tiles)),
            dma((3, tiles)),
            dma((len(side),)),
            dma((len(side),)),
            dma((2,)),
            dma((2,)),
        ],
        compiler_params=pltpu.CompilerParams(
            collective_id=0, has_side_effects=True, vmem_limit_bytes=62 * 2**20
        ),
    )(*operands)


def fits_fused(fs_size, tp_size, arrays):
    shards = [a for i, a in enumerate(arrays) if i in (2, 3, 4, 6, 7, 13, 15, 16, 17)]
    rows_fit = all(a.shape[0] % 16 == 0 for a in shards)
    lanes_fit = all(arrays[i].shape[1] % 128 == 0 for i in (0, 6, 7))
    lanes_fit = lanes_fit and arrays[17].shape[1] > 128
    tiles_fit = arrays[0].shape[0] % (2 * TILE) == 0 and arrays[2].shape[1] % 32 == 0
    turned_fit = all(arrays[i].shape[0] % 128 == 0 for i in (2, 3, 15, 16))
    return (
        rows_fit
        and lanes_fit
        and tiles_fit
        and turned_fit
        and fs_size % 2 == 0
        and 6 <= fs_size <= 16
        and tp_size == 4
    )


def local(
    tokens,
    pre_gain,
    pre_gate,
    pre_up,
    pre_down,
    mix_gain,
    branch_proj,
    gate_proj,
    conv_taps,
    retain_blocks,
    admit_blocks,
    decay_param,
    channel_gain,
    out_proj,
    post_gain,
    post_gate,
    post_up,
    post_down,
):
    after_pre = feed_forward(tokens, pre_gain, pre_gate, pre_up, pre_down)
    after_mix = recurrent_mixer(
        after_pre,
        mix_gain,
        branch_proj,
        gate_proj,
        conv_taps,
        retain_blocks,
        admit_blocks,
        decay_param,
        channel_gain,
        out_proj,
    )
    return feed_forward(after_mix, post_gain, post_gate, post_up, post_down)


def solution(mesh):
    placed = (
        P("fs", "tp"),
        P(),
        P("fs", "tp"),
        P("fs", "tp"),
        P("fs", "tp"),
        P(),
        P("fs", "tp"),
        P("fs", "tp"),
        P(None, "tp"),
        P("tp", None, None),
        P("tp", None, None),
        P("tp"),
        P(),
        P("fs", "tp"),
        P(),
        P("fs", "tp"),
        P("fs", "tp"),
        P("fs", "tp"),
    )
    fs_size, tp_size = mesh.shape["fs"], mesh.shape["tp"]

    def layer(*arrays):
        if fits_fused(fs_size, tp_size, arrays):
            return fused(fs_size, tp_size, *arrays)
        return local(*arrays)

    return jax.shard_map(
        layer, mesh=mesh, in_specs=placed, out_specs=P("fs", "tp"), check_vma=False
    )
```

```python
import functools

import jax
import jax.numpy as jnp
from jax import lax
from jax.experimental import pallas as pl
from jax.experimental.pallas import tpu as pltpu
from jax.sharding import PartitionSpec as P

SEQ_LEN = 128


EPSILON = 1e-06
DECAY_SCALE = 8.0


def normalize(values, norm_gain):
    floats = values.astype(jnp.float32)
    scaled = floats * lax.rsqrt(jnp.mean(floats * floats, axis=-1, keepdims=True) + EPSILON)
    return (scaled * norm_gain).astype(jnp.bfloat16)


def widen(residual):
    return lax.all_gather(residual, "tp", axis=1, tiled=True)


def contract(operand, stacked):
    return jnp.dot(
        operand,
        lax.all_gather(stacked.astype(jnp.bfloat16), "fs", axis=0, tiled=True),
        preferred_element_type=jnp.float32,
    )


def feed_forward(residual, norm_gain, gate_matrix, up_matrix, down_matrix):
    normed = normalize(widen(residual), norm_gain)
    products = contract(normed, jnp.concatenate((gate_matrix, up_matrix), axis=1))
    split_at = gate_matrix.shape[1]
    hidden = (jax.nn.silu(products[:, :split_at]) * products[:, split_at:]).astype(jnp.bfloat16)
    all_hidden = lax.all_gather(hidden, "tp", axis=1, tiled=True)
    return (residual.astype(jnp.float32) + 0.5 * contract(all_hidden, down_matrix)).astype(
        jnp.bfloat16
    )


def shifted(values, distance, fill):
    row = lax.broadcasted_iota(jnp.int32, values.shape, 0)
    return jnp.where(row >= distance, pltpu.roll(values, distance, 0), fill)


def mix_sequence(branch, gate_act, taps, gates, sharpness):
    width = branch.shape[1]
    count = taps.shape[0]
    convolved = branch * taps[count - 1 : count]
    for back in range(1, count):
        convolved = convolved + shifted(branch, back, 0.0) * taps[count - 1 - back : count - back]
    convolved = convolved.astype(jnp.bfloat16)
    both = jax.nn.sigmoid(jnp.dot(convolved, gates, preferred_element_type=jnp.float32))
    log_keep = -DECAY_SCALE * both[:, :width] * sharpness
    keep = jnp.exp(log_keep)
    inject = (
        jnp.sqrt(jnp.tanh(-log_keep) * (1.0 + keep * keep))
        * both[:, width:]
        * convolved.astype(jnp.float32)
    )
    distance = 1
    while distance < branch.shape[0]:
        inject = keep * shifted(inject, distance, 0.0) + inject
        keep = keep * shifted(keep, distance, 1.0)
        distance *= 2
    return (inject * jax.nn.gelu(gate_act)).astype(jnp.bfloat16)


def mix_kernel(products_ref, taps_ref, gates_ref, sharp_ref, out_ref):
    width = out_ref.shape[1]
    out_ref[...] = mix_sequence(
        products_ref[:, :width],
        products_ref[:, width:],
        taps_ref[...],
        gates_ref[...],
        sharp_ref[...],
    )


def spread_blocks(blocks):
    count, size, _ = blocks.shape
    eye = jnp.eye(count, dtype=blocks.dtype)
    wide = eye[:, None, :, None] * blocks[:, :, None, :]
    return wide.reshape(count * size, count * size).astype(jnp.bfloat16)


def recurrent_mixer(
    residual,
    norm_gain,
    branch_matrix,
    gate_matrix,
    conv_taps,
    retain_blocks,
    admit_blocks,
    decay_param,
    channel_gain,
    out_matrix,
):
    normed = normalize(widen(residual), norm_gain)
    products = contract(normed, jnp.concatenate((branch_matrix, gate_matrix), axis=1))
    width = branch_matrix.shape[1]
    rows = residual.shape[0]
    gates = jnp.concatenate((spread_blocks(retain_blocks), spread_blocks(admit_blocks)), axis=1)
    sharpness = jax.nn.softplus(-decay_param)[None, :]
    whole = lambda array: pl.BlockSpec(array.shape, lambda i: (0, 0))
    mixed_rows = pl.pallas_call(
        mix_kernel,
        grid=(rows // SEQ_LEN,),
        in_specs=[
            pl.BlockSpec((SEQ_LEN, 2 * width), lambda i: (i, 0)),
            whole(conv_taps),
            whole(gates),
            whole(sharpness),
        ],
        out_specs=pl.BlockSpec((SEQ_LEN, width), lambda i: (i, 0)),
        out_shape=jax.ShapeDtypeStruct((rows, width), jnp.bfloat16),
        cost_estimate=pl.CostEstimate(
            flops=rows * width * 1200, bytes_accessed=rows * width * 10, transcendentals=0
        ),
    )(products, conv_taps, gates, sharpness)
    all_channels = lax.all_gather(mixed_rows, "tp", axis=1, tiled=True)
    mixed_normed = normalize(all_channels, channel_gain)
    return (residual.astype(jnp.float32) + contract(mixed_normed, out_matrix)).astype(jnp.bfloat16)


TILE = SEQ_LEN
TAKEN = 3
MESH = pl.DeviceIdType.MESH


def when(condition, action):
    if condition is None:
        action()
    else:
        pl.when(condition)(action)


class Exchange:
    def __init__(self):
        self.sent = []

    def send(self, source, target, send_sem, recv_sem, device, condition=None):
        copy = remote(source, target, send_sem, recv_sem, device)
        when(condition, copy.start)
        self.sent.append((copy, condition))

    def drain(self):
        for copy, condition in self.sent:
            when(condition, copy.wait_send)


def remote(source, target, send_sem, recv_sem, device):
    return pltpu.make_async_remote_copy(
        src_ref=source,
        dst_ref=target,
        send_sem=send_sem,
        recv_sem=recv_sem,
        device_id=device,
        device_id_type=MESH,
    )


def softplus(values):
    return jnp.maximum(values, 0.0) + jnp.log1p(jnp.exp(-jnp.abs(values)))


def layer_kernel(fs_size, tp_size, *refs):
    (tokens_in, pre_gain, mix_gain, channel_gain, post_gain) = refs[:5]
    own_side = refs[5:9]
    matrices = refs[9:18]
    out = refs[18]
    refs = refs[19:]
    whole = refs[:9]
    shards = refs[9:18]
    raw = refs[18:27]
    refs = refs[2:]
    first, second, third, channels = refs[25:29]
    hidden_one, hidden_two = refs[29:31], refs[31:33]
    normed, final, gates = refs[33:36]
    refs = refs[1:]
    side = refs[35:39]
    recv_sem, twin_sem, pace_sem, own_sem, take_sem, swap_sem, raw_sem = refs[39:46]
    token_sem, token_recv, token_pass = refs[46:49]
    slot_recv, slot_sem = refs[49:51]
    side_sem, side_recv, out_sem, out_recv = refs[51:55]
    tokens, tokens_sem = refs[55:57]
    taps, retain, admit, decay = side

    f = lax.axis_index("fs")
    t = lax.axis_index("tp")
    x = lax.rem(f, 2)
    z = f // 2
    y = t // 2
    c = lax.rem(t, 2)
    depth = fs_size // 2
    home = x == c
    away = x != c
    end = (z == 0) | (z == depth - 1)
    inner = (z > 0) & (z < depth - 1)

    mine = 2 * y + x
    beside = 2 * y + 1 - x
    behind = 2 * (1 - y) + x
    corner = 2 * (1 - y) + 1 - x
    line = 2 * z + c

    across = f + 1 - 2 * x
    other = t + 1 - 2 * c
    x_peer = {"fs": across}
    y_peer = {"tp": lax.rem(t + 2, tp_size)}
    twin = {"tp": other}
    partner = {"fs": across, "tp": other}
    skew = {"tp": lax.rem(other + 2, tp_size)}
    above = {"fs": lax.rem(f + 2, fs_size)}
    below = {"fs": lax.rem(f + fs_size - 2, fs_size)}
    links = Exchange()

    def load(m):
        return pltpu.make_async_copy(matrices[m], raw[m], raw_sem.at[m])

    tokens_copy = pltpu.make_async_copy(tokens_in, tokens, tokens_sem)
    for m in range(2):
        load(m).start()
    tokens_copy.start()
    for m in range(2, len(matrices)):
        load(m).start()

    def convert(p):
        parts = {0: (0, 1), 2: (2,), 3: (3, 4), 4: (5,), 5: (6, 7), 7: (8,)}.get(p, ())
        at = 0
        for m in parts:
            load(m).wait()
            if p in (0, 5):
                half = raw[m].shape[0] // 2
                for k in range(2):
                    shards[p + k][at : at + half, :] = raw[m][
                        k * half : (k + 1) * half, :
                    ].astype(jnp.bfloat16)
                at += half
            elif p == 7:
                cut = shards[7].shape[1]
                shards[7][...] = raw[m][:, :cut].astype(jnp.bfloat16)
                shards[8][...] = raw[m][:, cut:].astype(jnp.bfloat16)
            else:
                shards[p][:, at : at + raw[m].shape[1]] = raw[m][...].astype(jnp.bfloat16)
                at += raw[m].shape[1]

    barrier = pltpu.get_barrier_semaphore()
    greeted = [
        (x_peer, None),
        (y_peer, None),
        (twin, None),
        (partner, None),
        (skew, None),
        (above, z < depth - 1),
        (below, z > 0),
    ]
    expected = 0
    for device, condition in greeted:
        when(
            condition,
            functools.partial(
                pl.semaphore_signal, barrier, inc=1, device_id=device, device_id_type=MESH
            ),
        )
        expected = expected + (1 if condition is None else condition.astype(jnp.int32))
    convert(0)
    pl.semaphore_wait(barrier, expected)

    def block(p, owner):
        rows = shards[p].shape[0]
        return whole[p].at[pl.ds(pl.multiple_of(owner * rows, rows), rows)]

    def arrive(p, level, condition=None):
        place = block(p, 2 * level + c)
        copy = remote(place, place, own_sem.at[p, 0], recv_sem.at[p, level], twin)
        when(condition, copy.wait_recv)

    def arrive_twin(p, blocks, sem, condition=None):
        place = whole[p].at[pl.ds(0, blocks * shards[p].shape[0])]
        copy = remote(place, place, own_sem.at[p, 0], sem, twin)
        when(condition, copy.wait_recv)

    def swap(p):
        links.send(shards[p], block(p, f), swap_sem.at[p], recv_sem.at[p, z], partner, away)
        when(home, pltpu.make_async_copy(shards[p], block(p, f), swap_sem.at[p]).start)

    def settle(p, who=None):
        if who is None or who == "home":
            when(home, pltpu.make_async_copy(shards[p], block(p, f), swap_sem.at[p]).wait)
        if who is None or who == "away":
            arrive(p, z, away)

    def launch(p, who):
        place, sem = block(p, line), recv_sem.at[p, z]
        links.send(place, place, own_sem.at[p, 1], sem, above, who & (z < depth - 2))
        links.send(place, place, own_sem.at[p, 2], sem, below, who & (z > 1))
        sem = pace_sem if p == 0 else twin_sem.at[p]
        links.send(place, place, own_sem.at[p, 0], sem, twin, who)

    def launch_last(p, who):
        place, sem = block(p, line), recv_sem.at[p, z]
        links.send(place, place, own_sem.at[p, 1], sem, above, who & (z == depth - 2))
        links.send(place, place, own_sem.at[p, 2], sem, below, who & (z == 1))

    taken = {}

    def take(p, key, level, condition):
        for copy, earlier in taken.get((p - TAKEN, key), ()):
            when(condition & earlier, copy.wait_send)
        arrive(p, level, condition)
        place = block(p, 2 * level + c)
        sends = (
            (recv_sem.at[p, level], above, condition & (z < depth - 1) & (level < z)),
            (recv_sem.at[p, level], below, condition & (z > 0) & (level > z)),
            (twin_sem.at[p], twin, condition),
        )
        for k, (sem, device, who) in enumerate(sends):
            copy = remote(place, place, take_sem.at[p % TAKEN, k, level], sem, device)
            when(who, copy.start)
            taken.setdefault((p, key), []).append((copy, who))

    def pump(p, condition, distances=None):
        for distance in distances or range(1, depth):
            for sign in (-1, 1):
                level = z + sign * distance
                exists = (level >= 0) & (level < depth)
                take(p, sign * distance, lax.rem(level + depth, depth), condition & exists)

    def near(p):
        pump(p, inner, (1,))

    def far(p):
        pump(p, inner, range(2, depth))

    def ready(p):
        pump(p, end)
        if p == 0:
            arrive_twin(p, 1, pace_sem, away)
            arrive_twin(p, depth - 1, twin_sem.at[p])
        else:
            arrive_twin(p, depth, twin_sem.at[p])

    def tile_rows(s):
        return pl.ds(pl.multiple_of(s * TILE, TILE), TILE)

    def tile_sends(array, index, s):
        odd = lax.rem(s, 2)
        place = array.at[mine, tile_rows(s)]
        return (
            remote(
                place, place, slot_sem.at[0, s], slot_recv.at[index - 1, 1 - odd, s], x_peer
            ),
            remote(place, place, slot_sem.at[1, s], slot_recv.at[index - 1, odd, s], y_peer),
        )

    def tile_pass(array, index, s, kind):
        odd = lax.rem(s, 2)
        slot = behind * (1 - odd) + beside * odd
        place = array.at[slot, tile_rows(s)]
        device = {
            "fs": f + (1 - odd) * (1 - 2 * x),
            "tp": lax.rem(t + 2 * odd, tp_size),
        }
        return remote(place, place, slot_sem.at[2, s], slot_recv.at[index - 1, kind, s], device)

    gathered = (None, *hidden_one, second, channels, third, *hidden_two)

    def emit(array, index, s):
        if index > 1:
            for copy in tile_sends(gathered[index - 1], index - 1, s):
                copy.wait_send()
        for copy in tile_sends(array, index, s):
            copy.start()

    def relay(array, index, s):
        if index > 1:
            tile_pass(gathered[index - 1], index - 1, s, 1).wait_send()
        tile_pass(array, index, s, 0).wait_recv()
        tile_pass(array, index, s, 1).start()

    def complete(array, index, s):
        place = array.at[pl.ds(0, 2), tile_rows(s)]
        remote(
            place, place, slot_sem.at[0, s], slot_recv.at[index - 1, 1, s], x_peer
        ).wait_recv()

    total_rows = tokens.shape[0]
    tiles = total_rows // TILE

    def loop(body):
        def run(s, carry):
            body(s)
            return carry

        lax.fori_loop(0, tiles, run, 0)

    def stage(index, array, work, earlier=None, before=()):
        def body(s):
            for k, ready_array in before:
                complete(ready_array, k, s)
            work(s)
            emit(array, index, s)
            if earlier is not None:
                k, ready_array = earlier
                pl.when(s == 0)(lambda: relay(ready_array, k, tiles - 1))
            pl.when(s > 0)(lambda: relay(array, index, s - 1))

        loop(body)

    def norm_rows(array, gain, s):
        width = array.shape[2]
        features = width * tp_size
        for piece in range(0, TILE, 64):
            rows = pl.ds(pl.multiple_of(s * TILE + piece, 64), 64)
            parts = [array[k, rows, :].astype(jnp.float32) for k in range(tp_size)]
            squares = sum(jnp.sum(part * part, axis=-1, keepdims=True) for part in parts)
            scale = lax.rsqrt(squares / features + EPSILON)
            for k, part in enumerate(parts):
                at = slice(k * width, (k + 1) * width)
                normed[rows, at] = (part * scale * gain[:, at]).astype(jnp.bfloat16)

    def dot(left, right):
        return jnp.dot(left, right, preferred_element_type=jnp.float32)

    def turned(rows, matrix, part):
        features = matrix.shape[1]
        width = matrix.shape[0] // fs_size
        half = width // 2
        return sum(
            lax.dot_general(
                normed[rows, k * features : (k + 1) * features],
                matrix[k * width + part * half : k * width + (part + 1) * half, :],
                (((1,), (1,)), ((), ())),
                preferred_element_type=jnp.float32,
            )
            for k in range(fs_size)
        )

    def hidden_tile(matrix, hidden):
        def work(s):
            rows = tile_rows(s)
            product = jax.nn.silu(turned(rows, matrix, 0)) * turned(rows, matrix, 1)
            hidden[mine, rows, :] = product.astype(jnp.bfloat16)

        return work

    def lowered(halves, down, residual, rows, columns):
        half = halves[0].shape[2]
        total = sum(
            dot(
                hidden[k, rows, :],
                down[(2 * k + part) * half : (2 * k + part + 1) * half, :],
            )
            for k in range(tp_size)
            for part, hidden in enumerate(halves)
        )
        value = residual[mine, rows, columns].astype(jnp.float32) + 0.5 * total
        return value.astype(jnp.bfloat16)

    def down_tile(s):
        rows = tile_rows(s)
        second[mine, rows, :] = lowered(
            hidden_one, whole[2], first, rows, slice(None)
        )

    def mix_tile(s):
        rows = tile_rows(s)
        norm_rows(second, mix_gain, s)
        width = channels.shape[2]
        products = dot(normed[rows, :], whole[3][...])
        channels[mine, rows, :] = mix_sequence(
            products[:, :width], products[:, width:], taps[...], gates[...], softplus(-decay[...])
        )

    def out_tile(s):
        rows = tile_rows(s)
        norm_rows(channels, channel_gain, s)
        width = channels.shape[2] * tp_size
        total = dot(normed[rows, :width], whole[4][...])
        third[mine, rows, :] = (second[mine, rows, :].astype(jnp.float32) + total).astype(
            jnp.bfloat16
        )

    cut = shards[7].shape[1]
    last_columns = (slice(0, cut), slice(cut, cut + shards[8].shape[1]))

    def out_send(part, rows):
        place = (rows, last_columns[part])
        return remote(
            final.at[place], out.at[place], out_sem.at[part], out_recv.at[part], partner
        )

    def out_keep(part, rows):
        place = (rows, last_columns[part])
        return pltpu.make_async_copy(final.at[place], out.at[place], out_sem.at[part])

    def spread(blocks, at):
        size = blocks.shape[1]
        for k in range(blocks.shape[0]):
            place = slice(k * size, (k + 1) * size)
            gates[place, at + k * size : at + (k + 1) * size] = blocks[k].astype(jnp.bfloat16)

    count = len(shards)
    gates[...] = jnp.zeros_like(gates)

    def token_arrive(slot, condition):
        place = first.at[slot]
        copy = remote(place, place, token_sem.at[1], token_recv.at[slot], y_peer)
        when(condition, copy.wait_recv)

    def token_cross(who):
        links.send(
            tokens,
            first.at[t],
            token_sem.at[1],
            token_recv.at[t],
            {"fs": across, "tp": 2 * y + x},
            who,
        )

    def side_copies():
        for k, (own, target) in enumerate(zip(own_side, side)):
            yield (
                remote(own, target, side_sem.at[k], side_recv.at[k], partner),
                pltpu.make_async_copy(own, target, side_sem.at[k]),
            )

    swap(0)
    tokens_copy.wait()
    keep_tokens = pltpu.make_async_copy(tokens, first.at[t], token_sem.at[0])
    when(home, keep_tokens.start)
    target, sem = first.at[t], token_recv.at[t]
    links.send(tokens, target, token_sem.at[2], sem, {"tp": behind})
    links.send(tokens, target, token_sem.at[3], sem, twin, away)
    settle(0, "home")
    launch(0, home)
    launch_last(0, home)
    convert(1)
    swap(1)
    token_cross(away)
    settle(1, "home")
    launch_last(1, home)
    launch(1, home & end)
    for p in range(2, 4):
        convert(p)
        swap(p)
        settle(p, "home")
        launch_last(p, home)
    arrive_twin(0, 1, pace_sem, home)
    token_cross(home)
    settle(0, "away")
    launch(0, away)
    launch_last(0, away)
    pump(0, inner & home)
    launch(1, home & inner)
    for p in range(4, count):
        convert(p)
        swap(p)
    for p in range(4, count):
        settle(p, "home")
    launch(2, home & inner)
    settle(1, "away")
    launch_last(1, away)
    launch(1, away & end)
    pump(0, inner & away)
    launch(1, away & inner)
    for k in range(2):
        slot = 2 * y + k
        token_arrive(slot, away)
        links.send(
            first.at[slot],
            first.at[slot],
            token_pass.at[k],
            token_recv.at[slot],
            y_peer,
            away,
        )
    for away_copy, home_copy in side_copies():
        when(away, away_copy.start)
        when(home, home_copy.start)
    when(home, keep_tokens.wait)
    token_arrive(other, home)
    token_arrive(2 * (1 - y), home)
    token_arrive(2 * (1 - y) + 1, home)
    for p in range(2, count):
        launch(p, home & end)
    near(1)
    for p in range(2, 4):
        settle(p, "away")
        launch(p, away)
    launch(3, home & inner)
    token_arrive(2 * (1 - y), away)
    token_arrive(2 * (1 - y) + 1, away)
    loop(functools.partial(norm_rows, first, pre_gain))
    far(1)
    launch_last(2, away & inner)
    launch_last(3, away & inner)
    ready(0)
    stage(1, hidden_one[0], hidden_tile(whole[0], hidden_one[0]))
    for p in range(4, count):
        settle(p, "away")
        launch(p, away & end)
    near(2)
    launch_last(4, inner)
    launch(4, inner)
    launch(5, inner)
    relay(hidden_one[0], 1, tiles - 1)
    far(2)
    near(3)
    ready(1)
    stage(2, hidden_one[1], hidden_tile(whole[1], hidden_one[1]))
    far(3)
    near(4)
    launch_last(5, inner)
    launch(6, inner)
    relay(hidden_one[1], 2, tiles - 1)
    far(4)
    near(5)
    for away_copy, home_copy in side_copies():
        when(away, away_copy.wait)
        when(home, home_copy.wait)
    spread(retain, 0)
    spread(admit, gates.shape[0])
    ready(2)
    stage(3, second, down_tile, before=((1, hidden_one[0]), (2, hidden_one[1])))
    far(5)
    launch_last(6, inner)
    near(6)
    launch(7, inner)
    launch(8, inner)
    ready(3)
    stage(4, channels, mix_tile, earlier=(3, second), before=((3, second),))
    far(6)
    launch_last(7, inner)
    launch_last(8, inner)
    near(7)
    near(8)
    ready(4)
    stage(5, third, out_tile, earlier=(4, channels), before=((4, channels),))
    far(7)
    far(8)
    relay(third, 5, tiles - 1)
    ready(5)
    post_tile = hidden_tile(whole[5], hidden_two[0])

    def post_norm_tile(s):
        norm_rows(third, post_gain, s)
        post_tile(s)

    stage(6, hidden_two[0], post_norm_tile, before=((5, third),))
    relay(hidden_two[0], 6, tiles - 1)
    ready(6)
    stage(7, hidden_two[1], hidden_tile(whole[6], hidden_two[1]))
    relay(hidden_two[1], 7, tiles - 1)
    size = 2 * TILE
    for part in range(2):
        ready(7 + part)

        def last_rows(i, part=part):
            rows = pl.ds(pl.multiple_of(i * size, size), size)
            if part == 0:
                for k in range(2):
                    complete(hidden_two[0], 6, 2 * i + k)
                    complete(hidden_two[1], 7, 2 * i + k)
            final[rows, last_columns[part]] = lowered(
                hidden_two, whole[7 + part], third, rows, last_columns[part]
            )
            when(away, out_send(part, rows).start)
            when(home, out_keep(part, rows).start)

        lax.fori_loop(0, total_rows // size, lambda i, carry: (last_rows(i), carry)[1], 0)

    links.drain()
    for (p, _), entries in taken.items():
        for copy, condition in entries if p >= count - TAKEN else ():
            when(condition, copy.wait_send)

    def drain_tiles(s):
        for copy in tile_sends(gathered[-1], len(gathered) - 1, s):
            copy.wait_send()
        tile_pass(gathered[-1], len(gathered) - 1, s, 1).wait_send()

    loop(drain_tiles)
    everything = pl.ds(0, total_rows)
    for part in range(2):
        when(away, out_send(part, everything).wait)
        when(home, out_keep(part, everything).wait)


def fused(
    fs_size,
    tp_size,
    tokens,
    pre_gain,
    pre_gate,
    pre_up,
    pre_down,
    mix_gain,
    branch_proj,
    gate_proj,
    conv_taps,
    retain_blocks,
    admit_blocks,
    decay_param,
    channel_gain,
    out_proj,
    post_gain,
    post_gate,
    post_up,
    post_down,
):
    matrices = [
        pre_gate.T,
        pre_up.T,
        pre_down,
        branch_proj,
        gate_proj,
        out_proj,
        post_gate.T,
        post_up.T,
        post_down,
    ]
    last = post_down.shape[1] - 128
    shards = [
        pre_gate.shape[::-1],
        pre_gate.shape[::-1],
        pre_down.shape,
        (branch_proj.shape[0], branch_proj.shape[1] + gate_proj.shape[1]),
        out_proj.shape,
        post_gate.shape[::-1],
        post_gate.shape[::-1],
        (post_down.shape[0], last),
        (post_down.shape[0], 128),
    ]
    rows, width = tokens.shape
    hidden = pre_gate.shape[1]
    channels = branch_proj.shape[1]
    side = [conv_taps, retain_blocks, admit_blocks, decay_param[None]]
    operands = [
        tokens,
        pre_gain[None],
        mix_gain[None],
        channel_gain[None],
        post_gain[None],
        *side,
        *matrices,
    ]
    dma = pltpu.SemaphoreType.DMA
    count = len(shards)
    depth = fs_size // 2
    tiles = rows // TILE
    stacked = lambda columns: pltpu.VMEM((tp_size, rows, columns), jnp.bfloat16)
    return pl.pallas_call(
        functools.partial(layer_kernel, fs_size, tp_size),
        out_shape=pltpu.VMEM(tokens.shape, tokens.dtype),
        in_specs=[pl.BlockSpec(memory_space=pl.ANY)]
        + [pl.BlockSpec(memory_space=pltpu.VMEM)] * (4 + len(side))
        + [pl.BlockSpec(memory_space=pl.ANY)] * len(matrices),
        out_specs=pl.BlockSpec(memory_space=pltpu.VMEM),
        scratch_shapes=[
            *(pltpu.VMEM((fs_size * s[0], s[1]), jnp.bfloat16) for s in shards),
            *(pltpu.VMEM(s, jnp.bfloat16) for s in shards),
            *(pltpu.VMEM(m.shape, m.dtype) for m in matrices),
            stacked(width),
            stacked(width),
            stacked(width),
            stacked(channels),
            stacked(hidden // 2),
            stacked(hidden // 2),
            stacked(hidden // 2),
            stacked(hidden // 2),
            pltpu.VMEM((rows, width * tp_size), jnp.bfloat16),
            pltpu.VMEM((rows, width), jnp.bfloat16),
            pltpu.VMEM((channels, 2 * channels), jnp.bfloat16),
            *(pltpu.VMEM(s.shape, s.dtype) for s in side),
            dma((count, depth)),
            dma((count,)),
            dma,
            dma((count, 3)),
            dma((TAKEN, 3, depth)),
            dma((count,)),
            dma((len(matrices),)),
            dma((4,)),
            dma((tp_size,)),
            dma((2,)),
            dma((7, 2, tiles)),
            dma((3, tiles)),
            dma((len(side),)),
            dma((len(side),)),
            dma((2,)),
            dma((2,)),
            pltpu.VMEM(tokens.shape, tokens.dtype),
            dma,
        ],
        compiler_params=pltpu.CompilerParams(
            collective_id=0, has_side_effects=True, vmem_limit_bytes=62 * 2**20
        ),
    )(*operands)


def fits_fused(fs_size, tp_size, arrays):
    shards = [a for i, a in enumerate(arrays) if i in (2, 3, 4, 6, 7, 13, 15, 16, 17)]
    rows_fit = all(a.shape[0] % 16 == 0 for a in shards)
    lanes_fit = all(arrays[i].shape[1] % 128 == 0 for i in (0, 6, 7))
    lanes_fit = lanes_fit and arrays[17].shape[1] > 128
    tiles_fit = arrays[0].shape[0] % (2 * TILE) == 0 and arrays[2].shape[1] % 32 == 0
    turned_fit = all(arrays[i].shape[0] % 128 == 0 for i in (2, 3, 15, 16))
    return (
        rows_fit
        and lanes_fit
        and tiles_fit
        and turned_fit
        and fs_size % 2 == 0
        and 6 <= fs_size <= 16
        and tp_size == 4
    )


def local(
    tokens,
    pre_gain,
    pre_gate,
    pre_up,
    pre_down,
    mix_gain,
    branch_proj,
    gate_proj,
    conv_taps,
    retain_blocks,
    admit_blocks,
    decay_param,
    channel_gain,
    out_proj,
    post_gain,
    post_gate,
    post_up,
    post_down,
):
    after_pre = feed_forward(tokens, pre_gain, pre_gate, pre_up, pre_down)
    after_mix = recurrent_mixer(
        after_pre,
        mix_gain,
        branch_proj,
        gate_proj,
        conv_taps,
        retain_blocks,
        admit_blocks,
        decay_param,
        channel_gain,
        out_proj,
    )
    return feed_forward(after_mix, post_gain, post_gate, post_up, post_down)


def solution(mesh):
    placed = (
        P("fs", "tp"),
        P(),
        P("fs", "tp"),
        P("fs", "tp"),
        P("fs", "tp"),
        P(),
        P("fs", "tp"),
        P("fs", "tp"),
        P(None, "tp"),
        P("tp", None, None),
        P("tp", None, None),
        P("tp"),
        P(),
        P("fs", "tp"),
        P(),
        P("fs", "tp"),
        P("fs", "tp"),
        P("fs", "tp"),
    )
    fs_size, tp_size = mesh.shape["fs"], mesh.shape["tp"]

    def layer(*arrays):
        if fits_fused(fs_size, tp_size, arrays):
            return fused(fs_size, tp_size, *arrays)
        return local(*arrays)

    return jax.shard_map(
        layer, mesh=mesh, in_specs=placed, out_specs=P("fs", "tp"), check_vma=False
    )
```
